512 devices in a mesh: ep: 32 (over z, core), tp: 16 (over y, x).
Axes of the slice: x: 4, y: 4, z: 16, core: 2. Of those that a mesh axis runs over, the one named last changes fastest.
Arguments:
- value_in: bfloat16 [32768, 1536], P('ep', 'tp'), may hold values from -6 to 6
- gate_in: bfloat16 [32768, 1536], P('ep', 'tp'), may hold values from -9 to 9
- conv_kernel: float32 [31, 1536], P(None, 'tp'), may hold values from -40 to 40
- norm_gain: float32 [1536], replicated, may hold values from 0.1 to 1.9
- norm_shift: float32 [1536], replicated, may hold values from -3 to 3
- out_weight: bfloat16 [1536, 2048], P(None, 'tp'), may hold values from -0.15625 to 0.15625
- expert_input: bfloat16 [6144, 2048], P('ep'), may hold values from -6 to 6
- expert_gain: float32 [2048], replicated, may hold values from 0.1 to 1.9
- route_ids: int32 [6144, 4], P('ep'), may hold values from 0 to 31, all different within a row; in each aligned block of 192 rows (0 to 191, 192 to 383, ...) at most 30 rows name the same one
- route_weights: float32 [6144, 4], P('ep'), may hold values from 0.2 to 1
- gate_weight: bfloat16 [32, 2048, 2048], P('ep', None, 'tp'), may hold values from -0.375 to 0.375
- up_weight: bfloat16 [32, 2048, 2048], P('ep', None, 'tp'), may hold values from -0.375 to 0.375
- down_weight: bfloat16 [32, 2048, 2048], P('ep', None, 'tp'), may hold values from -0.01953125 to 0.01953125
Outputs:
- mixed_out: bfloat16 [32768, 2048], P('ep', 'tp')
- routed_out: bfloat16 [6144, 2048], P('ep', 'tp')
The draws below stay inside these ranges and needn't reach their ends.
Inputs may be any that keep to these rules, and one draw needn't show every extreme that they name: `route_ids`: each row names 4 different experts; among the rows of one index of ep (aligned blocks of 192 rows) no expert is named by more than 30 rows, and in some block one expert is named by exactly 30.
All inputs are finite; a program needn't handle non-finite values.
Results may differ from the reference program's by a relative error of at most 0.0071.
Values may be sent and summed in bfloat16 or wider, within the bound.
A program may use at most 64 MiB of HBM per device.

```python
import math
import jax
import jax.numpy as jnp
import numpy as np
from jax import lax

D = 2048
CH = 1536
FF = 2048
KW = 31
TOPK = 4
TOK_B = 192
EXPERTS = 32
CAP = 30
LENGTH = 32768
TOKENS_B = 6144
N_EP = 32


def draw_conv_kernel(key, part):
    first_key, second_key = jax.random.split(jax.random.fold_in(key, 17), 2)
    channel = jnp.arange(CH, dtype=jnp.float32) / CH
    jitter = jax.random.uniform(second_key, (CH,), jnp.float32, 0.0, 1.0)
    entries = jnp.clip(jax.random.normal(first_key, (KW, CH), jnp.float32), -4.0, 4.0)
    scales = 10.0 ** channel * 2.0 ** jitter
    return (entries * scales[None, :] * KW ** (-0.5)).astype(jnp.float32)


def steps_of(rng, extent, pieces, smallest, top_value):
    def one(dim, blocks):
        draws = jax.random.uniform(jax.random.fold_in(jax.random.fold_in(rng, 6), dim), (blocks,), jnp.float32, smallest / len(pieces), top_value / len(pieces))
        return jnp.repeat(jnp.exp(draws), extent[dim] // blocks).reshape((-1,) + (1,) * (len(extent) - dim - 1))

    factor_of = one(*pieces[0])
    for cut in pieces[1:]:
        factor_of = factor_of * one(*cut)
    return factor_of


def assign_block(key, own, number, rows, number_of, top, bound, lean):
    sequence = jax.random.permutation(key, number_of)
    packed, common = portions_of(number_of, rows * top, bound, lean, True), portions_of(number_of, rows * top, bound, lean, False)
    places = jnp.arange(number_of)

    def named(tallies, turn):
        used = int((tallies > 0).sum())
        fixed = max(1, used // 4)
        passed = fixed + (places - fixed + turn * (used - fixed)) % max(1, number_of - fixed)
        return jnp.zeros((number_of,), jnp.int32).at[sequence[jnp.where(places < fixed, places, passed)]].set(jnp.asarray(tallies, jnp.int32))

    tallies = jnp.where(number % 4 == 0, named(packed, number // 4), named(common, number - number // 4 - 1))
    mixed = jax.random.permutation(jax.random.fold_in(own, 3), number_of)
    donor, receiver = mixed[0:number_of // 2 * 2:2], mixed[1:number_of // 2 * 2:2]
    margin = jnp.minimum(tallies[donor] - 1, bound - tallies[receiver]) // 2
    margin = jnp.where((donor == sequence[0]) | (receiver == sequence[0]) | (tallies[receiver] == 0), 0, jnp.maximum(margin, 0))
    passed = jax.random.randint(jax.random.fold_in(own, 4), (number_of // 2,), 0, 1 << 20) % (margin + 1)
    tallies = tallies.at[donor].add(-passed).at[receiver].add(passed)
    members = jnp.searchsorted(jnp.cumsum(tallies), jnp.arange(rows * top), side="right").astype(jnp.int32)
    grid = members.reshape(top, rows).T
    grid = grid[jax.random.permutation(jax.random.fold_in(own, 1), rows)]
    turn = jax.random.randint(jax.random.fold_in(own, 2), (rows, 1), 0, top)
    return jnp.take_along_axis(grid, (jnp.arange(top)[None, :] + turn) % top, axis=1)


def portions_of(amount, total, limit, skew, full):
    portions = [(1 << 20) // math.isqrt(rank ** skew) + 1 for rank in range(1, amount + 1)]
    largest = limit if full else min(limit, max(-(-total // amount), total * portions[0] // sum(portions)))
    least = 1 if total - largest >= amount - 1 else 0
    given, rest = [largest] + [least] * (amount - 1), total - largest - least * (amount - 1)
    while rest > 0:
        free = [i for i in range(1, amount) if given[i] < largest] or [i for i in range(1, amount) if given[i] < limit]
        pool, remaining = sum([portions[i] for i in free]), rest
        for i in free:
            extra = min(limit - given[i], max(1, remaining * portions[i] // pool), rest)
            given[i] = given[i] + extra
            rest = rest - extra
    return np.array(given)


def gaussian(own_key, shape, width, limit, cuts=(), kind=jnp.bfloat16):
    values = jax.random.normal(own_key, shape, jnp.float32) * width
    if len(cuts) > 0:
        values = steps_of(own_key, shape, cuts, -0.22, 0.18) * values
    return jnp.clip(values, min=-limit, max=limit).astype(kind)


def setup_inputs(seed: int = 0) -> dict:
    key_list = jax.random.split(jax.random.key(seed), 14)
    value_in = gaussian(key_list[0], (LENGTH, CH), 1.0, 6.0, ((0, 32), (1, 16)))
    gate_in = gaussian(key_list[1], (LENGTH, CH), 1.5, 9.0, ((0, 32), (1, 16)))
    conv_kernel = draw_conv_kernel(jax.random.fold_in(key_list[13], 71), 0)
    norm_gain = jnp.clip(1.0 + 0.18 * jax.random.normal(key_list[3], (CH,), jnp.float32), 0.1, 1.9)
    norm_shift = gaussian(key_list[4], (CH,), 0.5, 3.0, (), jnp.float32)
    out_weight = gaussian(key_list[5], (CH, D), CH ** -0.5, 0.15625, ((1, 16),))
    expert_input = gaussian(key_list[6], (TOKENS_B, D), 1.0, 6.0, ((0, 32),))
    expert_gain = jnp.clip(1.0 + 0.18 * jax.random.normal(key_list[7], (D,), jnp.float32), 0.1, 1.9)
    route_ids_keys = jax.random.split(jax.random.fold_in(key_list[8], 1), TOKENS_B // TOK_B)
    route_ids_turns = jax.random.permutation(jax.random.fold_in(key_list[8], 3), TOKENS_B // TOK_B)
    route_ids = jax.vmap(lambda own, number: assign_block(jax.random.fold_in(key_list[8], 2), own, number, TOK_B, EXPERTS, TOPK, CAP, 2))(route_ids_keys, route_ids_turns).reshape((TOKENS_B, TOPK))
    route_weights = jnp.clip(0.2 + 0.8 * jax.random.uniform(key_list[9], (TOKENS_B, TOPK), jnp.float32) ** steps_of(key_list[9], (TOKENS_B, TOPK), ((0, 32),), -0.2, 0.2), 0.2, 1.0)
    gate_weight = gaussian(key_list[10], (EXPERTS, D, FF), (D // 9) ** -0.5, 0.375, ((0, 32), (2, 16)))
    up_weight = gaussian(key_list[11], (EXPERTS, D, FF), (D // 9) ** -0.5, 0.375, ((0, 32), (2, 16)))
    down_weight = gaussian(key_list[12], (EXPERTS, FF, D), (45 * FF) ** -0.5, 0.01953125, ((0, 32), (2, 16)))
    return {"value_in": value_in, "gate_in": gate_in, "conv_kernel": conv_kernel, "norm_gain": norm_gain, "norm_shift": norm_shift, "out_weight": out_weight, "expert_input": expert_input, "expert_gain": expert_gain, "route_ids": route_ids, "route_weights": route_weights, "gate_weight": gate_weight, "up_weight": up_weight, "down_weight": down_weight}


def reference(value_in, gate_in, conv_kernel, norm_gain, norm_shift, out_weight, expert_input, expert_gain, route_ids, route_weights, gate_weight, up_weight, down_weight):
    gated_values = (value_in.astype(jnp.float32) * jax.nn.sigmoid(gate_in.astype(jnp.float32))).astype(jnp.bfloat16)
    kernel_width = conv_kernel.shape[0]
    positions = gated_values.shape[0]
    padded = jnp.concatenate([jnp.zeros((kernel_width - 1, gated_values.shape[1]), jnp.bfloat16), gated_values], 0)
    running = jnp.zeros(gated_values.shape, jnp.float32)
    for tap_index in range(kernel_width):
        running = running + conv_kernel[tap_index][None, :] * padded[tap_index:tap_index + positions].astype(jnp.float32)
    convolved = running.astype(jnp.bfloat16)
    conv_float = convolved.astype(jnp.float32)
    row_mean = lax.optimization_barrier(jnp.mean(conv_float, axis=1, keepdims=True))
    row_var = lax.optimization_barrier(jnp.mean(jnp.square(conv_float - row_mean), axis=1, keepdims=True))
    normed = (conv_float - row_mean) * lax.rsqrt(row_var + 1e-05) * norm_gain[None, :] + norm_shift[None, :]
    hidden = jax.nn.silu(normed).astype(jnp.bfloat16)
    mixed_out = jnp.dot(hidden, out_weight, preferred_element_type=jnp.float32).astype(jnp.bfloat16)
    input_float = expert_input.astype(jnp.float32)
    feature_mean = lax.optimization_barrier(jnp.mean(input_float, axis=1, keepdims=True))
    feature_var = lax.optimization_barrier(jnp.mean(jnp.square(input_float - feature_mean), axis=1, keepdims=True))
    normed_rows = ((input_float - feature_mean) * lax.rsqrt(feature_var + 1e-05) * expert_gain[None, :]).astype(jnp.bfloat16)
    row_total = expert_input.shape[0]
    block_ids = route_ids.reshape(N_EP, TOK_B * TOPK)
    onehot = (block_ids[:, :, None] == jnp.arange(EXPERTS, dtype=jnp.int32)[None, None, :]).astype(jnp.int32)
    earlier = jnp.cumsum(onehot, axis=1) - onehot
    position = lax.optimization_barrier(jnp.sum(earlier * onehot, axis=2))
    blocks = jnp.arange(N_EP, dtype=jnp.int32)[:, None]
    slot_index = (block_ids * (N_EP * CAP) + blocks * CAP + position).reshape(-1).astype(jnp.int32)
    token_index = jnp.arange(N_EP * TOK_B * TOPK, dtype=jnp.int32) // TOPK
    slot_table = jnp.full((EXPERTS * N_EP * CAP,), row_total, jnp.int32).at[slot_index].set(token_index)
    padded_rows = jnp.concatenate([normed_rows, jnp.zeros((1, normed_rows.shape[1]), jnp.bfloat16)], 0)

    def run_expert(operands):
        table_rows, gate_matrix, up_matrix, down_matrix = operands
        slot_rows = padded_rows[table_rows]
        gate_pre = jnp.dot(slot_rows, gate_matrix, preferred_element_type=jnp.float32)
        up_pre = jnp.dot(slot_rows, up_matrix, preferred_element_type=jnp.float32)
        clamped = jnp.minimum(gate_pre, 7.0)
        upward = jnp.clip(up_pre, -7.0, 7.0)
        activation = ((upward + 1.0) * clamped * jax.nn.sigmoid(1.702 * clamped)).astype(jnp.bfloat16)
        return jnp.dot(activation, down_matrix, preferred_element_type=jnp.float32).astype(jnp.bfloat16)
    results = lax.map(run_expert, (slot_table.reshape(EXPERTS, N_EP * CAP), gate_weight, up_weight, down_weight))
    picked = results.reshape(-1, results.shape[2])[slot_index].reshape(row_total, TOPK, -1).astype(jnp.float32)
    routed_out = lax.optimization_barrier(jnp.sum(picked * route_weights[:, :, None], axis=1)).astype(jnp.bfloat16)
    return (mixed_out, routed_out)
```

```python
import functools
import jax
import jax.numpy as jnp
from jax import lax
from jax.experimental import pallas as pl
from jax.experimental.pallas import tpu as pltpu
from jax.sharding import PartitionSpec as P

MESH = pl.DeviceIdType.MESH
NX = 4
NY = 4
NTP = NX * NY
NEP = 32
SLOT = 32


class TpGather:
    def __init__(self, src, buf, send, recv, base, row0=0, rows=None):
        self.src, self.buf, self.send_sem, self.recv_sem, self.base = src, buf, send, recv, base
        self.row0 = row0
        self.rows = buf.shape[1] if rows is None else rows
        tp = lax.axis_index("tp")
        self.tp, self.y, self.x = tp, tp // NX, lax.rem(tp, NX)
        self.sent = []

    def at(self, dy, dx):
        return lax.rem(self.y + (dy + NY), NY) * NX + lax.rem(self.x + (dx + NX), NX)

    def rel(self, h, first, second):
        return self.at(second, first) if h == 0 else self.at(first, second)

    def span(self, h, part):
        half = self.rows // 2
        if part is None:
            return pl.ds(self.row0 + h * half, half)
        return pl.ds(self.row0 + h * half + part * (half // 2), half // 2)

    def sem(self, h, phase, k, n):
        return self.base + h * 20 + (n if phase == 0 else 4 + 4 * k + n)

    def push(self, h, phase, k, first, second, part, direction):
        n = (0 if direction > 0 else 1) + (0 if part is None else 2)
        own = first == 0 and second == 0
        shard = self.rel(h, first, second)
        span = self.span(h, part)
        source = self.src.at[span] if own else self.buf.at[shard, span]
        to = self.rel(h, direction, 0) if phase == 0 else self.rel(h, 0, direction)
        i = self.sem(h, phase, k, n)
        copy = pltpu.make_async_remote_copy(
            src_ref=source,
            dst_ref=self.buf.at[shard, span],
            send_sem=self.send_sem.at[i],
            recv_sem=self.recv_sem.at[i],
            device_id={"tp": to},
            device_id_type=MESH,
        )
        copy.start()
        self.sent.append(copy)

    def arrive(self, h, phase, k, n):
        off = (-1, 1, 2, 2)[n]
        part = None if n < 2 else n - 2
        first = (0, -1, 1, 2)[k] if phase else off
        second = off if phase else 0
        span = self.span(h, part)
        place = self.buf.at[self.rel(h, first, second), span]
        i = self.sem(h, phase, k, n)
        pltpu.make_async_remote_copy(
            src_ref=place,
            dst_ref=place,
            send_sem=self.send_sem.at[i],
            recv_sem=self.recv_sem.at[i],
            device_id={"tp": self.at(0, 1)},
            device_id_type=MESH,
        ).wait_recv()

    def both(self, h, phase, k, first):
        self.push(h, phase, k, first, 0, None, 1)
        self.push(h, phase, k, first, 0, None, -1)

    def relay(self, h, phase, k, n):
        self.arrive(h, phase, k, n)
        off = (-1, 1)[n]
        first = (0, -1, 1, 2)[k] if phase else off
        second = off if phase else 0
        self.push(h, phase, k, first, second, n, -off)

    def start(self):
        for h in (0, 1):
            self.both(h, 0, 0, 0)
        for h in (0, 1):
            self.both(h, 1, 0, 0)

    def stage(self, s):
        if s == 0:
            for n in (0, 1):
                for h in (0, 1):
                    self.relay(h, 0, 0, n)
            for k in (1, 2):
                for h in (0, 1):
                    self.both(h, 1, k, (0, -1, 1, 2)[k])
        elif s == 1:
            for n in (0, 1):
                for h in (0, 1):
                    self.relay(h, 1, 0, n)
            for h in (0, 1):
                self.arrive(h, 0, 0, 2)
                self.arrive(h, 0, 0, 3)
                self.both(h, 1, 3, 2)
        elif s == 2:
            for k in (1, 2):
                for n in (0, 1):
                    for h in (0, 1):
                        self.relay(h, 1, k, n)
        elif s == 3:
            for n in (0, 1):
                for h in (0, 1):
                    self.relay(h, 1, 3, n)
        elif s == 4:
            for k in range(4):
                for n in (2, 3):
                    for h in (0, 1):
                        self.arrive(h, 1, k, n)

    def finish(self):
        for copy in self.sent:
            copy.wait_send()


def greet_plane():
    barrier = pltpu.get_barrier_semaphore()
    tp = lax.axis_index("tp")
    y, x = tp // NX, lax.rem(tp, NX)
    for dy, dx in ((0, 1), (0, 3), (1, 0), (3, 0)):
        to = lax.rem(y + dy, NY) * NX + lax.rem(x + dx, NX)
        pl.semaphore_signal(barrier, inc=1, device_id={"tp": to}, device_id_type=MESH)
    pl.semaphore_wait(barrier, 4)


def gather_kernel(src, buf, send, recv):
    greet_plane()
    gather = TpGather(src, buf, send, recv, 0)
    gather.start()
    buf[gather.tp] = src[...]
    for s in range(5):
        gather.stage(s)
    gather.finish()


def tp_gather(shard, number):
    rows, cols = shard.shape
    return pl.pallas_call(
        gather_kernel,
        out_shape=jax.ShapeDtypeStruct((NTP, rows, cols), shard.dtype),
        in_specs=[pl.BlockSpec(memory_space=pltpu.VMEM)],
        out_specs=pl.BlockSpec(memory_space=pltpu.VMEM),
        scratch_shapes=[pltpu.SemaphoreType.DMA((40,)), pltpu.SemaphoreType.DMA((40,))],
        compiler_params=pltpu.CompilerParams(collective_id=number, has_side_effects=True),
        name="tp_gather",
    )(shard)


def exchange_kernel(src, dst, send, recv):
    barrier = pltpu.get_barrier_semaphore()
    me = lax.axis_index("ep")
    for d in range(1, NEP):
        pl.semaphore_signal(
            barrier, inc=1, device_id={"ep": lax.rem(me + d, NEP)}, device_id_type=MESH
        )
    pl.semaphore_wait(barrier, NEP - 1)
    sent = []
    for d in sorted(range(1, NEP), key=lambda d: -min(d, NEP - d)):
        to = lax.rem(me + d, NEP)
        copy = pltpu.make_async_remote_copy(
            src_ref=src.at[to],
            dst_ref=dst.at[me],
            send_sem=send.at[d],
            recv_sem=recv.at[d],
            device_id={"ep": to},
            device_id_type=MESH,
        )
        copy.start()
        sent.append(copy)
    dst[me] = src[me]
    for d in range(1, NEP):
        came = lax.rem(me + NEP - d, NEP)
        pltpu.make_async_remote_copy(
            src_ref=dst.at[came],
            dst_ref=dst.at[came],
            send_sem=send.at[d],
            recv_sem=recv.at[d],
            device_id={"ep": came},
            device_id_type=MESH,
        ).wait_recv()
    for copy in sent:
        copy.wait_send()


def ep_exchange(blocks, number):
    return pl.pallas_call(
        exchange_kernel,
        out_shape=jax.ShapeDtypeStruct(blocks.shape, blocks.dtype),
        in_specs=[pl.BlockSpec(memory_space=pltpu.VMEM)],
        out_specs=pl.BlockSpec(memory_space=pltpu.VMEM),
        scratch_shapes=[pltpu.SemaphoreType.DMA((NEP,)), pltpu.SemaphoreType.DMA((NEP,))],
        compiler_params=pltpu.CompilerParams(collective_id=number, has_side_effects=True),
        name="ep_exchange",
    )(blocks)


def body(
    value_in,
    gate_in,
    conv_kernel,
    norm_gain,
    norm_shift,
    out_weight,
    expert_input,
    expert_gain,
    route_ids,
    route_weights,
    gate_weight,
    up_weight,
    down_weight,
):
    f32, bf16 = jnp.float32, jnp.bfloat16
    rows, width = expert_input.shape
    cols = width // NTP
    tp = lax.axis_index("tp")
    experts = jnp.arange(NEP, dtype=jnp.int32)
    chosen = route_ids[:, :, None] == experts[None, None, :]
    onehot = jnp.any(chosen, axis=1)
    share = jnp.sum(jnp.where(chosen, route_weights[:, :, None], 0.0), axis=1)
    earlier = (jnp.arange(rows)[:, None] > jnp.arange(rows)[None, :]).astype(bf16)
    place = jnp.dot(earlier, onehot.astype(bf16), preferred_element_type=f32)
    place = jnp.where(onehot, place.astype(jnp.int32), -1)
    slots = jnp.arange(SLOT, dtype=jnp.int32)
    pick = (place.T[:, None, :] == slots[None, :, None]).astype(bf16).reshape(NEP * SLOT, rows)
    wide = expert_input.astype(f32)
    mean = jnp.mean(wide, axis=1, keepdims=True)
    var = jnp.mean(jnp.square(wide - mean), axis=1, keepdims=True)
    mine = lax.dynamic_slice_in_dim(expert_input, tp * cols, cols, 1).astype(f32)
    gain = lax.dynamic_slice_in_dim(expert_gain, tp * cols, cols, 0)
    normed = ((mine - mean) * lax.rsqrt(var + 1e-05) * gain[None, :]).astype(bf16)
    outgoing = jnp.dot(pick, normed, preferred_element_type=f32).astype(bf16)
    arrived = ep_exchange(outgoing.reshape(NEP, SLOT, cols), 0)
    gathered = tp_gather(arrived.reshape(NEP * SLOT, cols), 1)
    flat = jnp.transpose(gathered, (1, 0, 2)).reshape(NEP * SLOT, width)
    gate_pre = jnp.dot(flat, gate_weight[0], preferred_element_type=f32)
    up_pre = jnp.dot(flat, up_weight[0], preferred_element_type=f32)
    clamped = jnp.minimum(gate_pre, 7.0)
    upward = jnp.clip(up_pre, -7.0, 7.0)
    activation = ((upward + 1.0) * clamped * jax.nn.sigmoid(1.702 * clamped)).astype(bf16)
    acts = tp_gather(activation, 2)
    acts = jnp.transpose(acts, (1, 0, 2)).reshape(NEP * SLOT, width)
    outcome = jnp.dot(acts, down_weight[0], preferred_element_type=f32).astype(bf16)
    home = ep_exchange(outcome.reshape(NEP, SLOT, cols), 3).reshape(NEP * SLOT, cols)
    mix = jnp.where(place[:, :, None] == slots[None, None, :], share[:, :, None], 0.0)
    mix = mix.reshape(rows, NEP * SLOT)
    mix_hi = mix.astype(bf16)
    mix_lo = (mix - mix_hi.astype(f32)).astype(bf16)
    routed_out = (
        jnp.dot(mix_hi, home, preferred_element_type=f32)
        + jnp.dot(mix_lo, home, preferred_element_type=f32)
    ).astype(bf16)
    gated = (value_in.astype(f32) * jax.nn.sigmoid(gate_in.astype(f32))).astype(bf16)
    taps = conv_kernel.shape[0]
    length = gated.shape[0]
    n = lax.axis_size("ep")
    before = lax.ppermute(
        gated[length - (taps - 1) :], "ep", [(i, i + 1) for i in range(n - 1)]
    )
    extended = jnp.concatenate([before, gated], 0).astype(f32)
    running = jnp.zeros(gated.shape, f32)
    for j in range(taps):
        running = running + conv_kernel[j][None, :] * extended[j : j + length]
    convolved = jnp.pad(running.astype(bf16), ((0, 0), (0, 128 - gated.shape[1])))
    full = tp_gather(convolved, 4)[:, :, : gated.shape[1]]
    full = jnp.transpose(full, (1, 0, 2)).reshape(length, -1).astype(f32)
    row_mean = jnp.mean(full, axis=1, keepdims=True)
    row_var = jnp.mean(jnp.square(full - row_mean), axis=1, keepdims=True)
    scaled = (full - row_mean) * lax.rsqrt(row_var + 1e-05) * norm_gain[None, :] + norm_shift[None, :]
    hidden = jax.nn.silu(scaled).astype(bf16)
    mixed_out = jnp.dot(hidden, out_weight, preferred_element_type=f32).astype(bf16)
    return (mixed_out, routed_out)


def solution(mesh):
    return jax.shard_map(
        body,
        mesh=mesh,
        in_specs=(
            P("ep", "tp"),
            P("ep", "tp"),
            P(None, "tp"),
            P(),
            P(),
            P(None, "tp"),
            P("ep", None),
            P(),
            P("ep", None),
            P("ep", None),
            P("ep", None, "tp"),
            P("ep", None, "tp"),
            P("ep", None, "tp"),
        ),
        out_specs=(P("ep", "tp"), P("ep", "tp")),
        check_vma=False,
    )
```

```python
import jax
import jax.numpy as jnp
from jax import lax
from jax.experimental import pallas as pl
from jax.experimental.pallas import tpu as pltpu
from jax.sharding import PartitionSpec as P

MESH = pl.DeviceIdType.MESH
F32, BF16 = jnp.float32, jnp.bfloat16
NX = 4
NY = 4
NTP = NX * NY
NEP = 32
HALF = 16
OTHER = 14
TAPS = 31
OFFS = (0, -1, 1, 2)


def sigmoid(v):
    return 0.5 * jnp.tanh(0.5 * v) + 0.5


class TpGather:
    def __init__(self, buf, send, recv, base, axis):
        self.buf, self.send_sem, self.recv_sem, self.base, self.axis = buf, send, recv, base, axis
        self.size = buf.shape[1 + axis]
        tp = lax.axis_index("tp")
        self.tp, self.y, self.x = tp, tp // NX, lax.rem(tp, NX)
        self.sent = []

    def at(self, dy, dx):
        return lax.rem(self.y + (dy + NY), NY) * NX + lax.rem(self.x + (dx + NX), NX)

    def rel(self, h, first, second):
        return self.at(second, first) if h == 0 else self.at(first, second)

    def place(self, h, first, second, part):
        half = self.size // 2
        span = (
            pl.ds(h * half, half)
            if part is None
            else pl.ds(h * half + part * (half // 2), half // 2)
        )
        shard = self.rel(h, first, second)
        return self.buf.at[shard, span] if self.axis == 0 else self.buf.at[shard, :, span]

    def sem(self, h, phase, k, n):
        return self.base + h * 20 + (n if phase == 0 else 4 + 4 * k + n)

    def push(self, h, phase, k, first, second, part, direction):
        n = (0 if direction > 0 else 1) + (0 if part is None else 2)
        place = self.place(h, first, second, part)
        to = self.rel(h, direction, 0) if phase == 0 else self.rel(h, 0, direction)
        i = self.sem(h, phase, k, n)
        copy = pltpu.make_async_remote_copy(
            src_ref=place,
            dst_ref=place,
            send_sem=self.send_sem.at[i],
            recv_sem=self.recv_sem.at[i],
            device_id={"tp": to},
            device_id_type=MESH,
        )
        copy.start()
        self.sent.append(copy)

    def arrive(self, h, phase, k, n):
        off = (-1, 1, 2, 2)[n]
        part = None if n < 2 else n - 2
        first = OFFS[k] if phase else off
        second = off if phase else 0
        place = self.place(h, first, second, part)
        i = self.sem(h, phase, k, n)
        pltpu.make_async_remote_copy(
            src_ref=place,
            dst_ref=place,
            send_sem=self.send_sem.at[i],
            recv_sem=self.recv_sem.at[i],
            device_id={"tp": self.at(0, 1)},
            device_id_type=MESH,
        ).wait_recv()

    def both(self, h, phase, k, first):
        self.push(h, phase, k, first, 0, None, 1)
        self.push(h, phase, k, first, 0, None, -1)

    def relay(self, h, phase, k, n):
        self.arrive(h, phase, k, n)
        off = (-1, 1)[n]
        first = OFFS[k] if phase else off
        second = off if phase else 0
        self.push(h, phase, k, first, second, n, -off)

    def start(self):
        for h in (0, 1):
            self.both(h, 0, 0, 0)
        for h in (0, 1):
            self.both(h, 1, 0, 0)

    def stage(self, s):
        if s == 0:
            for n in (0, 1):
                for h in (0, 1):
                    self.relay(h, 0, 0, n)
            for k in (1, 2):
                for h in (0, 1):
                    self.both(h, 1, k, OFFS[k])
        elif s == 1:
            for n in (0, 1):
                for h in (0, 1):
                    self.relay(h, 1, 0, n)
            for h in (0, 1):
                self.arrive(h, 0, 0, 2)
                self.arrive(h, 0, 0, 3)
                self.both(h, 1, 3, 2)
        elif s == 2:
            for k in (1, 2):
                for n in (0, 1):
                    for h in (0, 1):
                        self.relay(h, 1, k, n)
        elif s == 3:
            for n in (0, 1):
                for h in (0, 1):
                    self.relay(h, 1, 3, n)
        else:
            for k in range(4):
                for n in (2, 3):
                    for h in (0, 1):
                        self.arrive(h, 1, k, n)

    def finish(self):
        for copy in self.sent:
            copy.wait_send()


class Exchange:
    def __init__(self, src, dst, send, recv, number):
        self.src, self.dst = src, dst
        self.send_sem, self.recv_sem = send.at[number], recv.at[number]
        self.me = lax.axis_index("ep")

    def block(self, ref, index):
        return ref.at[pl.ds(pl.multiple_of(index * HALF, HALF), HALF)]

    def start(self):
        me = self.me

        def one(d):
            to = lax.rem(me + d, NEP)
            pltpu.make_async_remote_copy(
                src_ref=self.block(self.src, to),
                dst_ref=self.block(self.dst, me),
                send_sem=self.send_sem,
                recv_sem=self.recv_sem,
                device_id={"ep": to},
                device_id_type=MESH,
            ).start()

        one(NEP // 2)

        def pair(i, carry):
            one(NEP // 2 - i)
            one(NEP // 2 + i)
            return carry

        lax.fori_loop(1, NEP // 2, pair, 0)
        own = pl.ds(pl.multiple_of(me * HALF, HALF), HALF)
        self.dst[own] = self.src[own]

    def all_of(self):
        span = pl.ds(0, (NEP - 1) * HALF)
        return pltpu.make_async_remote_copy(
            src_ref=self.src.at[span],
            dst_ref=self.dst.at[span],
            send_sem=self.send_sem,
            recv_sem=self.recv_sem,
            device_id={"ep": lax.rem(self.me + 1, NEP)},
            device_id_type=MESH,
        )

    def arrive(self):
        self.all_of().wait_recv()

    def finish(self):
        self.all_of().wait_send()


def iota(shape, dim):
    return lax.broadcasted_iota(jnp.int32, shape, dim)


def dot(a, b):
    return jnp.dot(a, b, preferred_element_type=F32)


def conv_span(ext, taps_ref, cg, tp, channels, start, length):
    def group(g, carry):
        rows = pl.ds(pl.multiple_of(g * 16, 16), 16)
        wide = ext[rows, pl.ds(start - 128, length + 128)]
        taps = taps_ref[rows, :]
        total = jnp.zeros((16, length), F32)
        for j in range(TAPS):
            shift = TAPS - 1 - j
            moved = wide if shift == 0 else pltpu.roll(wide, shift, 1)
            total = total + taps[:, j : j + 1] * moved[:, 128:]
        cg[tp, rows, pl.ds(start - 128, length)] = total.astype(BF16)
        return carry

    lax.fori_loop(0, channels // 16, group, 0)


def kernel(
    value_ref,
    gate_ref,
    taps_ref,
    gain_ref,
    shift_ref,
    rows_ref,
    row_gain_ref,
    ids_ref,
    shares_ref,
    ow_hbm,
    wg_hbm,
    wu_hbm,
    wd_hbm,
    mixed_ref,
    routed_ref,
    ext,
    tail,
    halo,
    cg,
    out0,
    out1,
    arr1,
    x0,
    x1,
    h0,
    h1,
    y0,
    y1,
    r0,
    r1,
    ow,
    wgu,
    wd,
    load_sem,
    send,
    recv,
    zsend,
    zrecv,
    halo_sem,
):
    ep, tp = lax.axis_index("ep"), lax.axis_index("tp")
    channels, length = value_ref.shape
    count, width = rows_ref.shape
    cols = width // NTP

    barrier = pltpu.get_barrier_semaphore()
    y, x = tp // NX, lax.rem(tp, NX)
    for dy, dx in ((0, 1), (0, 3), (1, 0), (3, 0)):
        to = lax.rem(y + dy, NY) * NX + lax.rem(x + dx, NX)
        pl.semaphore_signal(barrier, inc=1, device_id={"tp": to}, device_id_type=MESH)

    def greet(d, carry):
        pl.semaphore_signal(
            barrier, inc=1, device_id={"ep": lax.rem(ep + d, NEP)}, device_id_type=MESH
        )
        return carry

    lax.fori_loop(1, NEP, greet, 0)

    loads = [
        pltpu.make_async_copy(wg_hbm.at[0], wgu.at[:, pl.ds(0, cols)], load_sem.at[0]),
        pltpu.make_async_copy(wu_hbm.at[0], wgu.at[:, pl.ds(cols, cols)], load_sem.at[1]),
        pltpu.make_async_copy(wd_hbm.at[0], wd, load_sem.at[2]),
        pltpu.make_async_copy(ow_hbm, ow, load_sem.at[3]),
    ]
    for load in loads:
        load.start()

    expert = iota((NEP, count), 0)
    chosen = jnp.zeros((NEP, count), F32)
    share = jnp.zeros((NEP, count), F32)
    for k in range(ids_ref.shape[0]):
        here = ids_ref[k : k + 1, :] == expert
        chosen = jnp.where(here, 1.0, chosen)
        share = jnp.where(here, shares_ref[k : k + 1, :], share)
    earlier = (iota((count, count), 0) < iota((count, count), 1)).astype(F32).astype(BF16)
    place = jnp.where(chosen > 0.5, dot(chosen.astype(BF16), earlier), -1.0)
    place_b = place.astype(BF16)
    total = jnp.zeros((count, cols), F32)
    for t in range(NTP):
        total = total + rows_ref[:, t * cols : (t + 1) * cols].astype(F32)
    mean = jnp.sum(total, axis=1, keepdims=True) * (1.0 / width)
    total = jnp.zeros((count, cols), F32)
    for t in range(NTP):
        off = rows_ref[:, t * cols : (t + 1) * cols].astype(F32) - mean
        total = total + off * off
    var = jnp.sum(total, axis=1, keepdims=True) * (1.0 / width)
    mine = rows_ref[:, pl.ds(pl.multiple_of(tp * cols, cols), cols)].astype(F32)
    normed = ((mine - mean) * lax.rsqrt(var + 1e-05) * row_gain_ref[pl.ds(tp, 1), :]).astype(BF16)
    spread = (lax.shift_right_logical(iota((NEP * HALF, NEP), 0), 4) == iota((NEP * HALF, NEP), 1))
    spread = spread.astype(F32).astype(BF16)
    slot_of = dot(spread, place_b)
    slot = jnp.bitwise_and(iota((NEP * HALF, count), 0), HALF - 1).astype(F32)
    for c, out in enumerate((out0, out1)):
        pick = (slot_of == slot + float(HALF * c)).astype(F32).astype(BF16)
        out[...] = dot(pick, normed).astype(BF16)

    gated = (value_ref[...].astype(F32) * sigmoid(gate_ref[...].astype(F32))).astype(BF16)
    tail[...] = gated[:, length - 128 :]
    ext[:, pl.ds(128, length)] = gated.astype(F32)
    conv_span(ext, taps_ref, cg, tp, channels, 256, length - 128)

    pl.semaphore_wait(barrier, 4 + NEP - 1)
    halo_copy = pltpu.make_async_remote_copy(
        src_ref=tail,
        dst_ref=halo,
        send_sem=halo_sem.at[0],
        recv_sem=halo_sem.at[1],
        device_id={"ep": lax.rem(ep + 1, NEP)},
        device_id_type=MESH,
    )
    halo_copy.start()
    go0 = Exchange(out0, x0.at[tp], zsend, zrecv, 0)
    go1 = Exchange(out1, arr1, zsend, zrecv, 1)
    go0.start()
    go1.start()
    halo_copy.wait_recv()
    ext[:, pl.ds(0, 128)] = jnp.where(ep > 0, halo[...].astype(F32), 0.0)
    conv_span(ext, taps_ref, cg, tp, channels, 128, 128)

    gc = TpGather(cg, send, recv, 0, 1)
    gx0 = TpGather(x0, send, recv, 40, 0)
    gx1 = TpGather(x1, send, recv, 80, 0)
    gh0 = TpGather(h0, send, recv, 120, 0)
    gh1 = TpGather(h1, send, recv, 160, 0)

    def up(xs, hs):
        n = xs.shape[1] // 2
        for i in range(2):
            lhs = jnp.concatenate([xs[t, i * n : (i + 1) * n, :] for t in range(NTP)], axis=1)
            pre = dot(lhs, wgu[...])
            g = jnp.minimum(pre[:, :cols], 7.0)
            u = jnp.clip(pre[:, cols:], -7.0, 7.0)
            hs[tp, pl.ds(i * n, n)] = ((u + 1.0) * g * sigmoid(1.702 * g)).astype(BF16)

    def down(hs):
        n = hs.shape[1] // 2
        parts = []
        for i in range(2):
            lhs = jnp.concatenate([hs[t, i * n : (i + 1) * n, :] for t in range(NTP)], axis=1)
            parts.append(dot(lhs, wd[...]).astype(BF16))
        return jnp.concatenate(parts, axis=0)

    few = NEP * OTHER

    def squeeze(shape, dim):
        row = iota(shape, dim).astype(F32)
        source = jnp.floor((row + 0.5) * (1.0 / OTHER))
        return row + source * float(HALF - OTHER)

    gc.start()
    gc.stage(0)
    go0.arrive()
    gx0.start()
    gc.stage(1)
    gx0.stage(0)
    go1.arrive()
    shrink = (squeeze((few, NEP * HALF), 0) == iota((few, NEP * HALF), 1).astype(F32)).astype(F32)
    x1[tp] = dot(shrink.astype(BF16), arr1[...]).astype(BF16)
    gc.stage(2)
    gx1.start()
    gx0.stage(1)
    gc.stage(3)
    gx1.stage(0)
    gx0.stage(2)
    gx1.stage(1)
    gx0.stage(3)
    loads[0].wait()
    loads[1].wait()
    gx0.stage(4)
    up(x0, h0)
    gh0.start()
    gx1.stage(2)
    gh0.stage(0)
    gx1.stage(3)
    gx1.stage(4)
    up(x1, h1)
    gh1.start()
    gh0.stage(1)
    gh1.stage(0)
    gh0.stage(2)
    gh1.stage(1)
    gh0.stage(3)
    loads[2].wait()
    gh0.stage(4)
    y0[...] = down(h0)
    back0 = Exchange(y0, r0, zsend, zrecv, 2)
    back0.start()
    gh1.stage(2)
    gh1.stage(3)
    gh1.stage(4)
    grow = (squeeze((NEP * HALF, few), 1) == iota((NEP * HALF, few), 0).astype(F32)).astype(F32)
    y1[...] = dot(grow.astype(BF16), down(h1)).astype(BF16)
    back1 = Exchange(y1, r1, zsend, zrecv, 3)
    back1.start()

    gc.stage(4)
    gc.finish()
    loads[3].wait()
    step = 256
    whole = NTP * channels
    turned = jnp.concatenate(
        [ow[i * 128 : (i + 1) * 128, :].T for i in range(whole // 128)], axis=1
    )

    def positions(i, carry):
        lanes = pl.ds(pl.multiple_of(i * step, step), step)
        acc = jnp.zeros((channels, step), F32)
        for t in range(NTP):
            acc = acc + cg[t, :, lanes].astype(F32)
        row_mean = jnp.sum(acc, axis=0, keepdims=True) * (1.0 / whole)
        acc = jnp.zeros((channels, step), F32)
        for t in range(NTP):
            off = cg[t, :, lanes].astype(F32) - row_mean
            acc = acc + off * off
        row_var = jnp.sum(acc, axis=0, keepdims=True) * (1.0 / whole)
        scale = lax.rsqrt(row_var + 1e-05)
        for t in range(NTP):
            part = slice(t * channels, (t + 1) * channels)
            v = (cg[t, :, lanes].astype(F32) - row_mean) * scale
            v = 0.5 * (v * gain_ref[part, :] + shift_ref[part, :])
            cg[t, :, lanes] = (v * jnp.tanh(v) + v).astype(BF16)
        hidden = jnp.concatenate([cg[t, :, lanes] for t in range(NTP)], axis=0)
        mixed = dot(turned, hidden)
        mixed_ref[lanes, :] = mixed.T.astype(BF16)
        return carry

    lax.fori_loop(0, length // step, positions, 0)

    def turn(a):
        eye = (iota((count, count), 0) == iota((count, count), 1)).astype(F32).astype(BF16)
        return lax.dot_general(eye, a, (((1,), (1,)), ((), ())), preferred_element_type=F32).astype(BF16)

    share_hi = share.astype(BF16)
    share_lo = (share - share_hi.astype(F32)).astype(BF16)
    widen = (lax.shift_right_logical(iota((NEP, NEP * HALF), 1), 4) == iota((NEP, NEP * HALF), 0))
    widen = widen.astype(F32).astype(BF16)
    slot_at = dot(turn(place_b), widen)
    hi_at = dot(turn(share_hi), widen)
    lo_at = dot(turn(share_lo), widen)
    slot = jnp.bitwise_and(iota((count, NEP * HALF), 1), HALF - 1).astype(F32)
    result = jnp.zeros((count, cols), F32)
    for c, (back, r) in enumerate(((back0, r0), (back1, r1))):
        back.arrive()
        there = slot_at == slot + float(HALF * c)
        result = result + dot(jnp.where(there, hi_at, 0.0).astype(BF16), r[...])
        result = result + dot(jnp.where(there, lo_at, 0.0).astype(BF16), r[...])
    routed_ref[...] = result.astype(BF16)

    halo_copy.wait_send()
    for moved in (go0, go1, gx0, gx1, gh0, gh1, back0, back1):
        moved.finish()


def body(
    value_in,
    gate_in,
    conv_kernel,
    norm_gain,
    norm_shift,
    out_weight,
    expert_input,
    expert_gain,
    route_ids,
    route_weights,
    gate_weight,
    up_weight,
    down_weight,
):
    length, channels = value_in.shape
    count, width = expert_input.shape
    cols = width // NTP
    few = NEP * OTHER
    many = NEP * HALF
    vmem = pl.BlockSpec(memory_space=pltpu.VMEM)
    hbm = pl.BlockSpec(memory_space=pltpu.HBM)
    mixed_out, routed_out = pl.pallas_call(
        kernel,
        out_shape=(
            jax.ShapeDtypeStruct((length, out_weight.shape[1]), BF16),
            jax.ShapeDtypeStruct((count, cols), BF16),
        ),
        in_specs=[vmem] * 9 + [hbm] * 4,
        out_specs=(vmem, vmem),
        scratch_shapes=[
            pltpu.VMEM((channels, 128 + length), F32),
            pltpu.VMEM((channels, 128), BF16),
            pltpu.VMEM((channels, 128), BF16),
            pltpu.VMEM((NTP, channels, length), BF16),
            pltpu.VMEM((many, cols), BF16),
            pltpu.VMEM((many, cols), BF16),
            pltpu.VMEM((many, cols), BF16),
            pltpu.VMEM((NTP, many, cols), BF16),
            pltpu.VMEM((NTP, few, cols), BF16),
            pltpu.VMEM((NTP, many, cols), BF16),
            pltpu.VMEM((NTP, few, cols), BF16),
            pltpu.VMEM((many, cols), BF16),
            pltpu.VMEM((many, cols), BF16),
            pltpu.VMEM((many, cols), BF16),
            pltpu.VMEM((many, cols), BF16),
            pltpu.VMEM(out_weight.shape, BF16),
            pltpu.VMEM((width, 2 * cols), BF16),
            pltpu.VMEM((width, cols), BF16),
            pltpu.SemaphoreType.DMA((4,)),
            pltpu.SemaphoreType.DMA((200,)),
            pltpu.SemaphoreType.DMA((200,)),
            pltpu.SemaphoreType.DMA((4,)),
            pltpu.SemaphoreType.DMA((4,)),
            pltpu.SemaphoreType.DMA((2,)),
        ],
        compiler_params=pltpu.CompilerParams(
            collective_id=0, has_side_effects=True, vmem_limit_bytes=60 * 1024 * 1024
        ),
        name="whole",
    )(
        value_in.T,
        gate_in.T,
        conv_kernel.T,
        norm_gain.reshape(-1, 1),
        norm_shift.reshape(-1, 1),
        expert_input,
        expert_gain.reshape(NTP, cols),
        route_ids.T,
        route_weights.T,
        out_weight,
        gate_weight,
        up_weight,
        down_weight,
    )
    return (mixed_out, routed_out)


def solution(mesh):
    return jax.shard_map(
        body,
        mesh=mesh,
        in_specs=(
            P("ep", "tp"),
            P("ep", "tp"),
            P(None, "tp"),
            P(),
            P(),
            P(None, "tp"),
            P("ep", None),
            P(),
            P("ep", None),
            P("ep", None),
            P("ep", None, "tp"),
            P("ep", None, "tp"),
            P("ep", None, "tp"),
        ),
        out_specs=(P("ep", "tp"), P("ep", "tp")),
        check_vma=False,
    )
```

```python
import jax
import jax.numpy as jnp
from jax import lax
from jax.experimental import pallas as pl
from jax.experimental.pallas import tpu as pltpu
from jax.sharding import PartitionSpec as P

MESH = pl.DeviceIdType.MESH
F32, BF16 = jnp.float32, jnp.bfloat16
NX = 4
NY = 4
NTP = NX * NY
NEP = 32
HALF = 16
OTHER = 14
TAPS = 31
UNROLL = 3
OFFS = (0, -1, 1, 2)

ORDER = (
    "c.S", "convB", "c.E00", "c.E01", "c.E10", "c.E11", "c.R000", "c.R001", "c.R100", "c.R101",
    "c.F0", "c.R010", "c.R011", "c.R110", "c.R111", "c.R020", "c.R021", "c.F1", "c.R120", "c.R121",
    "go0", "x.S", "c.R030", "c.R031", "c.R130", "c.R131", "x.E10", "x.E11", "x.E00", "x.E01",
    "x.R000", "x.R001", "x.R100", "x.R101", "go1", "y.S", "c.D", "projc0", "x.F1", "projc1",
    "x.R010", "x.R011", "x.R110", "x.R111", "x.R120", "x.R121", "x.R020", "x.R021", "x.F0", "y.E10",
    "y.E11", "y.E00", "y.E01", "y.R000", "y.R001", "y.R100", "y.R101", "x.R130", "x.R131", "x.R030",
    "x.R031", "y.F1", "y.R110", "y.R111", "y.R010", "y.R011", "y.R120", "y.R121", "y.R020", "y.R021",
    "y.F0", "x.D", "up0", "h.S", "y.R130", "y.R131", "y.R030", "y.R031", "h.E00", "h.E01",
    "h.E10", "h.E11", "h.R000", "h.R001", "h.R100", "h.R101", "y.D", "up1", "k.S", "h.F0",
    "h.R010", "h.R011", "h.R110", "h.R111", "h.R020", "h.R021", "h.F1", "h.R120", "h.R121", "k.E00",
    "k.E01", "k.E10", "k.E11", "k.R000", "k.R001", "k.R100", "k.R101", "h.R030", "h.R031", "h.R130",
    "h.R131", "k.F0", "k.R010", "k.R011", "k.R110", "k.R111", "k.R020", "k.R021", "k.F1", "k.R120",
    "k.R121", "h.D", "down0", "l.S", "k.R030", "k.R031", "k.R130", "k.R131", "l.E00", "l.E01",
    "l.E10", "l.E11", "l.R000", "l.R001", "l.R100", "l.R101", "k.D", "down1", "l.F0", "l.R010",
    "l.R011", "l.R110", "l.R111", "l.R020", "l.R021", "l.F1", "prep", "l.R120", "l.R121", "l.R030", "l.R031",
    "l.R130", "l.R131", "sum0", "l.D", "projl0", "projl1", "sum1",
)


def sigmoid(v):
    return 0.5 * jnp.tanh(0.5 * v) + 0.5


class TpGather:
    def __init__(self, buf, send, recv, number, axis):
        self.buf, self.axis = buf, axis
        self.height = buf.shape[0] // NTP
        self.size = self.height if axis == 0 else buf.shape[1]
        self.send_sem, self.recv_sem, self.base = send.at[number], recv, number * 23
        tp = lax.axis_index("tp")
        self.y, self.x = tp // NX, lax.rem(tp, NX)

    def at(self, dy, dx):
        return lax.rem(self.y + (dy + NY), NY) * NX + lax.rem(self.x + (dx + NX), NX)

    def rel(self, h, first, second):
        return self.at(second, first) if h == 0 else self.at(first, second)

    def place(self, h, first, second, part):
        half = self.size // 2
        start, size = (h * half, half) if part is None else (h * half + part * (half // 2), half // 2)
        row = self.rel(h, first, second) * self.height
        if self.axis == 0:
            return self.buf.at[pl.ds(pl.multiple_of(row + start, 16), size)]
        return self.buf.at[pl.ds(pl.multiple_of(row, 16), self.height), pl.ds(start, size)]

    def sem(self, h, phase, k, n):
        if phase == 0:
            return self.recv_sem.at[self.base + h * 11 + min(n, 2)]
        return self.recv_sem.at[self.base + (h * 11 + 3 + 2 * k + n if n < 2 else 22)]

    def wait(self, place, sem):
        pltpu.make_async_remote_copy(
            src_ref=place,
            dst_ref=place,
            send_sem=self.send_sem,
            recv_sem=sem,
            device_id={"tp": self.at(0, 1)},
            device_id_type=MESH,
        ).wait_recv()

    def push(self, h, phase, k, first, second, part, direction):
        n = (0 if direction > 0 else 1) + (0 if part is None else 2)
        place = self.place(h, first, second, part)
        to = self.rel(h, direction, 0) if phase == 0 else self.rel(h, 0, direction)
        pltpu.make_async_remote_copy(
            src_ref=place,
            dst_ref=place,
            send_sem=self.send_sem,
            recv_sem=self.sem(h, phase, k, n),
            device_id={"tp": to},
            device_id_type=MESH,
        ).start()

    def both(self, h, phase, k, first):
        self.push(h, phase, k, first, 0, None, 1)
        self.push(h, phase, k, first, 0, None, -1)

    def relay(self, h, phase, k, n):
        off = (-1, 1)[n]
        first = OFFS[k] if phase else off
        second = off if phase else 0
        self.wait(self.place(h, first, second, None), self.sem(h, phase, k, n))
        self.push(h, phase, k, first, second, n, -off)

    def start(self):
        for h in (0, 1):
            self.both(h, 0, 0, 0)
        for h in (0, 1):
            self.both(h, 1, 0, 0)

    def run(self, step):
        kind, index = step[0], [int(i) for i in step[1:]]
        if kind == "S":
            self.start()
        elif kind == "E":
            h, n = index
            self.relay(h, 0, 0, n)
            self.both(h, 1, n + 1, OFFS[n + 1])
        elif kind == "F":
            (h,) = index
            self.wait(self.place(h, 2, 0, None), self.sem(h, 0, 0, 2))
            self.both(h, 1, 3, 2)
        elif kind == "R":
            h, k, n = index
            self.relay(h, 1, k, n)
        else:
            self.wait(self.buf.at[pl.ds(0, 4 * self.height)], self.sem(0, 1, 0, 2))

    def finish(self):
        place = self.buf.at[pl.ds(0, (NTP - 1) * self.height)]
        pltpu.make_async_remote_copy(
            src_ref=place,
            dst_ref=place,
            send_sem=self.send_sem,
            recv_sem=self.sem(0, 1, 0, 2),
            device_id={"tp": self.at(0, 1)},
            device_id_type=MESH,
        ).wait_send()


class Exchange:
    def __init__(self, src, dst, send, recv, number):
        self.src, self.dst = src, dst
        self.send_sem, self.recv_sem = send.at[number], recv.at[number]
        self.me = lax.axis_index("ep")

    def block(self, ref, index):
        return ref.at[pl.ds(pl.multiple_of(index * HALF, HALF), HALF)]

    def start(self):
        me = self.me

        def one(d):
            to = lax.rem(me + d, NEP)
            pltpu.make_async_remote_copy(
                src_ref=self.block(self.src, to),
                dst_ref=self.block(self.dst, me),
                send_sem=self.send_sem,
                recv_sem=self.recv_sem,
                device_id={"ep": to},
                device_id_type=MESH,
            ).start()

        one(NEP // 2)

        def pair(i, carry):
            one(NEP // 2 - i)
            one(NEP // 2 + i)
            return carry

        lax.fori_loop(1, NEP // 2, pair, 0)
        own = pl.ds(pl.multiple_of(me * HALF, HALF), HALF)
        self.dst[own] = self.src[own]

    def all_of(self):
        span = pl.ds(0, (NEP - 1) * HALF)
        return pltpu.make_async_remote_copy(
            src_ref=self.src.at[span],
            dst_ref=self.dst.at[span],
            send_sem=self.send_sem,
            recv_sem=self.recv_sem,
            device_id={"ep": lax.rem(self.me + 1, NEP)},
            device_id_type=MESH,
        )

    def arrive(self):
        self.all_of().wait_recv()

    def finish(self):
        self.all_of().wait_send()


def iota(shape, dim):
    return lax.broadcasted_iota(jnp.int32, shape, dim)


def dot(a, b):
    return jnp.dot(a, b, preferred_element_type=F32)


def conv_span(ext, taps, cg, tp, channels, start, length):
    def group(g, carry):
        parts = []
        for u in range(2):
            rows = pl.ds(pl.multiple_of(g * 16, 16) + 8 * u, 8)
            wide = ext[rows, pl.ds(start - 128, length + 128)]
            tap = taps[rows, :]
            sums = [None] * 4
            for b in range(8):
                moved = pltpu.roll(wide, b, 1) if b else wide
                for a in range(4):
                    j = TAPS - 1 - (8 * a + b)
                    if j >= 0:
                        term = tap[:, j : j + 1] * moved
                        sums[a] = term if sums[a] is None else sums[a] + term
            total = sums[0]
            for a in range(1, 4):
                total = total + pltpu.roll(sums[a], 8 * a, 1)
            parts.append(total[:, 128:])
        own = pl.ds(pl.multiple_of(tp * channels + g * 16, 16), 16)
        cg[own, :] = jnp.concatenate(parts, axis=0).astype(BF16)
        return carry

    lax.fori_loop(0, channels // 16, group, 0, unroll=UNROLL)


def kernel(
    value_hbm,
    gate_hbm,
    taps_hbm,
    gain_hbm,
    shift_hbm,
    rows_hbm,
    row_gain_hbm,
    ids_hbm,
    shares_hbm,
    ow_hbm,
    wg_hbm,
    wu_hbm,
    wd_hbm,
    mixed_ref,
    routed_ref,
    value_ref,
    gate_ref,
    taps_ref,
    gain_ref,
    shift_ref,
    rows_ref,
    row_gain_ref,
    ids_ref,
    shares_ref,
    ext,
    taps,
    tap_pad,
    tail,
    halo,
    cg_late,
    cg,
    out0,
    out1,
    arr1,
    x0,
    x1,
    h0,
    h1,
    y0,
    y1,
    r0,
    r1,
    mix,
    ow,
    wgu,
    wd,
    load_sem,
    send,
    recv,
    zsend,
    zrecv,
    halo_sem,
):
    ep, tp = lax.axis_index("ep"), lax.axis_index("tp")
    channels, length = value_hbm.shape
    count, width = rows_hbm.shape
    cols = width // NTP

    barrier = pltpu.get_barrier_semaphore()
    y, x = tp // NX, lax.rem(tp, NX)
    for dy, dx in ((0, 1), (0, 3), (1, 0), (3, 0)):
        to = lax.rem(y + dy, NY) * NX + lax.rem(x + dx, NX)
        pl.semaphore_signal(barrier, inc=1, device_id={"tp": to}, device_id_type=MESH)

    def greet(d, carry):
        pl.semaphore_signal(
            barrier, inc=1, device_id={"ep": lax.rem(ep + d, NEP)}, device_id_type=MESH
        )
        return carry

    lax.fori_loop(1, NEP, greet, 0)

    pairs = (
        (ids_hbm, ids_ref),
        (shares_hbm, shares_ref),
        (rows_hbm, rows_ref),
        (row_gain_hbm, row_gain_ref),
        (value_hbm, value_ref),
        (gate_hbm, gate_ref),
        (taps_hbm, taps_ref),
        (gain_hbm, gain_ref),
        (shift_hbm, shift_ref),
        (ow_hbm, ow),
        (wg_hbm.at[0], wgu.at[:, pl.ds(0, cols)]),
        (wu_hbm.at[0], wgu.at[:, pl.ds(cols, cols)]),
        (wd_hbm.at[0], wd),
    )
    loads = [pltpu.make_async_copy(a, b, load_sem.at[i]) for i, (a, b) in enumerate(pairs)]
    for load in loads:
        load.start()
    for load in loads[:4]:
        load.wait()

    expert = iota((NEP, count), 0)
    chosen = jnp.zeros((NEP, count), F32)
    share = jnp.zeros((NEP, count), F32)
    for k in range(ids_ref.shape[0]):
        here = ids_ref[k : k + 1, :] == expert
        chosen = jnp.where(here, 1.0, chosen)
        share = jnp.where(here, shares_ref[k : k + 1, :], share)
    earlier = (iota((count, count), 0) < iota((count, count), 1)).astype(F32).astype(BF16)
    place = jnp.where(chosen > 0.5, dot(chosen.astype(BF16), earlier), -1.0)
    place_b = place.astype(BF16)
    total = jnp.zeros((count, cols), F32)
    for t in range(NTP):
        total = total + rows_ref[:, t * cols : (t + 1) * cols].astype(F32)
    mean = jnp.sum(total, axis=1, keepdims=True) * (1.0 / width)
    total = jnp.zeros((count, cols), F32)
    for t in range(NTP):
        off = rows_ref[:, t * cols : (t + 1) * cols].astype(F32) - mean
        total = total + off * off
    var = jnp.sum(total, axis=1, keepdims=True) * (1.0 / width)
    mine = rows_ref[:, pl.ds(pl.multiple_of(tp * cols, cols), cols)].astype(F32)
    normed = ((mine - mean) * lax.rsqrt(var + 1e-05) * row_gain_ref[pl.ds(tp, 1), :]).astype(BF16)
    spread = (lax.shift_right_logical(iota((NEP * HALF, NEP), 0), 4) == iota((NEP * HALF, NEP), 1))
    spread = spread.astype(F32).astype(BF16)
    slot_of = dot(spread, place_b)
    slot = jnp.bitwise_and(iota((NEP * HALF, count), 0), HALF - 1).astype(F32)
    for c, out in enumerate((out0, out1)):
        pick = (slot_of == slot + float(HALF * c)).astype(F32).astype(BF16)
        out[...] = dot(pick, normed).astype(BF16)

    for load in loads[4:7]:
        load.wait()
    gated = (value_ref[...].astype(F32) * sigmoid(gate_ref[...].astype(F32))).astype(BF16)
    tail[...] = gated[:, length - 128 :]
    ext[:, pl.ds(128, length)] = gated.astype(F32)
    tap_pad[pl.ds(0, TAPS), pl.ds(0, channels)] = taps_ref[...]
    taps[...] = tap_pad[...].T

    pl.semaphore_wait(barrier, 4 + NEP - 1)
    halo_copy = pltpu.make_async_remote_copy(
        src_ref=tail,
        dst_ref=halo,
        send_sem=halo_sem.at[0],
        recv_sem=halo_sem.at[1],
        device_id={"ep": lax.rem(ep + 1, NEP)},
        device_id_type=MESH,
    )
    halo_copy.start()
    go0 = Exchange(out0, x0.at[pl.ds(pl.multiple_of(tp * out0.shape[0], 16), out0.shape[0])], zsend, zrecv, 0)
    go1 = Exchange(out1, arr1, zsend, zrecv, 1)
    go0.start()
    go1.start()
    half = length // 2
    conv_span(ext, taps, cg, tp, channels, 128 + half, half)
    gathers = {
        name: TpGather(ref, send, recv, i, axis)
        for i, (name, ref, axis) in enumerate(
            (("c", cg, 1), ("l", cg_late, 1), ("x", x0, 0), ("y", x1, 0), ("h", h0, 0), ("k", h1, 0))
        )
    }
    back0 = Exchange(y0, r0, zsend, zrecv, 2)
    back1 = Exchange(y1, r1, zsend, zrecv, 3)

    def conv_late():
        halo_copy.wait_recv()
        ext[:, pl.ds(0, 128)] = jnp.where(ep > 0, halo[...].astype(F32), 0.0)
        conv_span(ext, taps, cg_late, tp, channels, 128, half)

    def wide_rows(ref, i):
        n = ref.shape[0] // NTP
        return jnp.concatenate(
            [ref[t * n + i * (n // 2) : t * n + (i + 1) * (n // 2), :] for t in range(NTP)], axis=1
        )

    def up(xs, hs):
        n = xs.shape[0] // NTP
        for i in range(2):
            pre = dot(wide_rows(xs, i), wgu[...])
            g = jnp.minimum(pre[:, :cols], 7.0)
            u = jnp.clip(pre[:, cols:], -7.0, 7.0)
            own = pl.ds(pl.multiple_of(tp * n + i * (n // 2), 16), n // 2)
            hs[own, :] = ((u + 1.0) * g * sigmoid(1.702 * g)).astype(BF16)

    def down(hs):
        parts = [dot(wide_rows(hs, i), wd[...]).astype(BF16) for i in range(2)]
        return jnp.concatenate(parts, axis=0)

    few = NEP * OTHER

    def squeeze(shape, dim):
        row = iota(shape, dim).astype(F32)
        source = jnp.floor((row + 0.5) * (1.0 / OTHER))
        return row + source * float(HALF - OTHER)

    def compact():
        go1.arrive()
        row, col = squeeze((few, NEP * HALF), 0), iota((few, NEP * HALF), 1).astype(F32)
        own = pl.ds(pl.multiple_of(tp * few, 16), few)
        x1[own, :] = dot((row == col).astype(F32).astype(BF16), arr1[...]).astype(BF16)

    def return_first():
        y0[...] = down(h0)
        back0.start()

    def return_second():
        row, col = iota((NEP * HALF, few), 0).astype(F32), squeeze((NEP * HALF, few), 1)
        y1[...] = dot((row == col).astype(F32).astype(BF16), down(h1)).astype(BF16)
        back1.start()

    whole = NTP * channels
    groups = whole // 128
    step = 256

    def project_ready():
        for load in loads[7:10]:
            load.wait()
        blank = jnp.zeros((16 - groups, 128), F32)
        gains = jnp.concatenate([gain_ref[...], blank], axis=0).T
        shifts = jnp.concatenate([shift_ref[...], blank], axis=0).T
        turned = jnp.concatenate([ow[i * 128 : (i + 1) * 128, :].T for i in range(groups)], axis=1)
        return gains, shifts, turned

    def project(buf, i, first, gains, shifts, turned):
        lanes = pl.ds(i * step, step)
        acc = jnp.zeros((128, step), F32)
        for t in range(groups):
            acc = acc + buf[t * 128 : (t + 1) * 128, lanes].astype(F32)
        row_mean = jnp.sum(acc, axis=0, keepdims=True) * (1.0 / whole)
        acc = jnp.zeros((128, step), F32)
        for t in range(groups):
            off = buf[t * 128 : (t + 1) * 128, lanes].astype(F32) - row_mean
            acc = acc + off * off
        row_var = jnp.sum(acc, axis=0, keepdims=True) * (1.0 / whole)
        scale = lax.rsqrt(row_var + 1e-05)
        for t in range(groups):
            v = (buf[t * 128 : (t + 1) * 128, lanes].astype(F32) - row_mean) * scale
            v = 0.5 * (v * gains[:, t : t + 1] + shifts[:, t : t + 1])
            buf[t * 128 : (t + 1) * 128, lanes] = (v * jnp.tanh(v) + v).astype(BF16)
        mixed = dot(turned, buf[:, lanes])
        mixed_ref[pl.ds(first + i * step, step), :] = mixed.T.astype(BF16)

    def turn(a):
        eye = (iota((count, count), 0) == iota((count, count), 1)).astype(F32).astype(BF16)
        return lax.dot_general(eye, a, (((1,), (1,)), ((), ())), preferred_element_type=F32).astype(BF16)

    def prepare():
        share_hi = share.astype(BF16)
        share_lo = (share - share_hi.astype(F32)).astype(BF16)
        shape = (NEP, NEP * HALF)
        widen = lax.shift_right_logical(iota(shape, 1), 4) == iota(shape, 0)
        widen = widen.astype(F32).astype(BF16)
        slot_at = dot(turn(place_b), widen)
        hi_at = dot(turn(share_hi), widen)
        lo_at = dot(turn(share_lo), widen)
        slot = jnp.bitwise_and(iota((count, NEP * HALF), 1), HALF - 1).astype(F32)
        for c in range(2):
            there = slot_at == slot + float(HALF * c)
            mix[2 * c] = jnp.where(there, hi_at, 0.0).astype(BF16)
            mix[2 * c + 1] = jnp.where(there, lo_at, 0.0).astype(BF16)

    def weigh(c, back, r):
        back.arrive()
        return dot(mix[2 * c], r[...]) + dot(mix[2 * c + 1], r[...])

    tables = None
    partial = None
    for step_name in ORDER:
        if "." in step_name:
            gathers[step_name[0]].run(step_name[2:])
        elif step_name == "convB":
            conv_late()
        elif step_name == "go0":
            go0.arrive()
        elif step_name == "go1":
            compact()
        elif step_name == "up0":
            loads[10].wait()
            loads[11].wait()
            up(x0, h0)
        elif step_name == "up1":
            up(x1, h1)
        elif step_name == "down0":
            loads[12].wait()
            return_first()
        elif step_name == "down1":
            return_second()
        elif step_name == "projc0":
            gathers["c"].finish()
            tables = project_ready()
            project(cg, 0, half, *tables)
        elif step_name == "projc1":
            project(cg, 1, half, *tables)
        elif step_name == "projl0":
            gathers["l"].finish()
            project(cg_late, 0, 0, *tables)
        elif step_name == "projl1":
            project(cg_late, 1, 0, *tables)
        elif step_name == "prep":
            prepare()
        elif step_name == "sum0":
            partial = weigh(0, back0, r0)
        else:
            routed_ref[...] = (partial + weigh(1, back1, r1)).astype(BF16)

    halo_copy.wait_send()
    for moved in (go0, go1, *(gathers[name] for name in "xyhk"), back0, back1):
        moved.finish()


def body(
    value_in,
    gate_in,
    conv_kernel,
    norm_gain,
    norm_shift,
    out_weight,
    expert_input,
    expert_gain,
    route_ids,
    route_weights,
    gate_weight,
    up_weight,
    down_weight,
):
    length, channels = value_in.shape
    count, width = expert_input.shape
    cols = width // NTP
    few = NEP * OTHER
    many = NEP * HALF
    vmem = pl.BlockSpec(memory_space=pltpu.VMEM)
    hbm = pl.BlockSpec(memory_space=pltpu.HBM)
    mixed_out, routed_out = pl.pallas_call(
        kernel,
        out_shape=(
            jax.ShapeDtypeStruct((length, out_weight.shape[1]), BF16),
            jax.ShapeDtypeStruct((count, cols), BF16),
        ),
        in_specs=[hbm] * 13,
        out_specs=(vmem, vmem),
        scratch_shapes=[
            pltpu.VMEM((channels, length), BF16),
            pltpu.VMEM((channels, length), BF16),
            pltpu.VMEM(conv_kernel.shape, F32),
            pltpu.VMEM((NTP * channels // 128, 128), F32),
            pltpu.VMEM((NTP * channels // 128, 128), F32),
            pltpu.VMEM((count, width), BF16),
            pltpu.VMEM((NTP, cols), F32),
            pltpu.VMEM(route_ids.shape[::-1], jnp.int32),
            pltpu.VMEM(route_ids.shape[::-1], F32),
            pltpu.VMEM((channels, 128 + length), F32),
            pltpu.VMEM((128, 32), F32),
            pltpu.VMEM((32, 128), F32),
            pltpu.VMEM((channels, 128), BF16),
            pltpu.VMEM((channels, 128), BF16),
            pltpu.VMEM((NTP * channels, length // 2), BF16),
            pltpu.VMEM((NTP * channels, length // 2), BF16),
            pltpu.VMEM((many, cols), BF16),
            pltpu.VMEM((many, cols), BF16),
            pltpu.VMEM((many, cols), BF16),
            pltpu.VMEM((NTP * many, cols), BF16),
            pltpu.VMEM((NTP * few, cols), BF16),
            pltpu.VMEM((NTP * many, cols), BF16),
            pltpu.VMEM((NTP * few, cols), BF16),
            pltpu.VMEM((many, cols), BF16),
            pltpu.VMEM((many, cols), BF16),
            pltpu.VMEM((many, cols), BF16),
            pltpu.VMEM((many, cols), BF16),
            pltpu.VMEM((4, count, many), BF16),
            pltpu.VMEM(out_weight.shape, BF16),
            pltpu.VMEM((width, 2 * cols), BF16),
            pltpu.VMEM((width, cols), BF16),
            pltpu.SemaphoreType.DMA((13,)),
            pltpu.SemaphoreType.DMA((6,)),
            pltpu.SemaphoreType.DMA((6 * 23,)),
            pltpu.SemaphoreType.DMA((4,)),
            pltpu.SemaphoreType.DMA((4,)),
            pltpu.SemaphoreType.DMA((2,)),
        ],
        compiler_params=pltpu.CompilerParams(
            collective_id=0, has_side_effects=True, vmem_limit_bytes=60 * 1024 * 1024
        ),
        name="whole",
    )(
        value_in.T,
        gate_in.T,
        conv_kernel,
        norm_gain.reshape(-1, 128),
        norm_shift.reshape(-1, 128),
        expert_input,
        expert_gain.reshape(NTP, cols),
        route_ids.T,
        route_weights.T,
        out_weight,
        gate_weight,
        up_weight,
        down_weight,
    )
    return (mixed_out, routed_out)


def solution(mesh):
    return jax.shard_map(
        body,
        mesh=mesh,
        in_specs=(
            P("ep", "tp"),
            P("ep", "tp"),
            P(None, "tp"),
            P(),
            P(),
            P(None, "tp"),
            P("ep", None),
            P(),
            P("ep", None),
            P("ep", None),
            P("ep", None, "tp"),
            P("ep", None, "tp"),
            P("ep", None, "tp"),
        ),
        out_specs=(P("ep", "tp"), P("ep", "tp")),
        check_vma=False,
    )
```

```python
import jax
import jax.numpy as jnp
from jax import lax
from jax.experimental import pallas as pl
from jax.experimental.pallas import tpu as pltpu
from jax.sharding import PartitionSpec as P

MESH = pl.DeviceIdType.MESH
F32, BF16 = jnp.float32, jnp.bfloat16
NX = 4
NY = 4
NTP = NX * NY
NEP = 32
HALF = 16
OTHER = 14
SLOTS = HALF + OTHER
NEAR = 10
FAR = 22
FAR_ROWS = FAR * HALF
LATE_ROWS = 320
NEAR_SEND = 32
NEAR_ROWS = 304
TAPS = 31
UNROLL = 6
OFFS = (0, -1, 1, 2)

ORDER = (
    0, 900, 10, 11, 12, 13, 20, 21, 28, 29, 2, 22, 23, 30, 31, 24,
    25, 3, 32, 33, 902, 200, 901, 26, 27, 34, 35, 212, 213, 210, 211, 220,
    221, 903, 300, 228, 229, 1, 910, 230, 231, 203, 911, 222, 223, 224, 225, 232,
    233, 202, 310, 311, 312, 313, 328, 329, 320, 321, 234, 235, 226, 227, 302, 322,
    323, 330, 331, 324, 325, 303, 332, 333, 914, 201, 904, 400, 326, 327, 334, 335,
    410, 411, 412, 413, 906, 420, 421, 428, 429, 301, 905, 500, 402, 422, 423, 430,
    431, 424, 425, 403, 432, 433, 510, 511, 512, 513, 600, 520, 521, 528, 529, 426,
    427, 434, 435, 502, 522, 523, 530, 531, 524, 525, 503, 532, 533, 610, 611, 612,
    613, 620, 621, 628, 629, 401, 907, 100, 526, 527, 534, 535, 602, 622, 623, 630,
    631, 624, 625, 603, 632, 633, 110, 111, 112, 113, 120, 121, 128, 129, 501, 908,
    626, 627, 634, 635, 102, 122, 123, 130, 131, 124, 125, 103, 132, 133, 601, 909,
    126, 127, 134, 135, 915, 101, 912, 913, 916, 917,
)


def sigmoid(v):
    return 0.5 * jnp.tanh(0.5 * v) + 0.5


class TpGather:
    def __init__(self, buf, send, recv, number, axis):
        self.buf, self.axis = buf, axis
        self.height = buf.shape[0] // NTP
        self.size = self.height if axis == 0 else buf.shape[1]
        self.send_sem, self.recv_sem, self.base = send.at[number], recv, number * 23
        unit = 16 if axis == 0 else 128
        whole = self.size // unit
        self.spans = {}
        for h, (at, size) in enumerate(((0, (whole + 1) // 2), ((whole + 1) // 2, whole // 2))):
            first = (size + 1) // 2
            self.spans[h, None] = (at * unit, size * unit)
            self.spans[h, 0] = (at * unit, first * unit)
            self.spans[h, 1] = ((at + first) * unit, (size - first) * unit)
        tp = lax.axis_index("tp")
        self.y, self.x = tp // NX, lax.rem(tp, NX)

    def at(self, dy, dx):
        return lax.rem(self.y + (dy + NY), NY) * NX + lax.rem(self.x + (dx + NX), NX)

    def rel(self, h, first, second):
        return self.at(second, first) if h == 0 else self.at(first, second)

    def place(self, h, first, second, part):
        start, size = self.spans[h, part]
        row = self.rel(h, first, second) * self.height
        if self.axis == 0:
            return self.buf.at[pl.ds(pl.multiple_of(row + start, 16), size)]
        return self.buf.at[pl.ds(pl.multiple_of(row, 16), self.height), pl.ds(start, size)]

    def sem(self, h, phase, k, n):
        if phase == 0:
            return self.recv_sem.at[self.base + h * 11 + min(n, 2)]
        return self.recv_sem.at[self.base + (h * 11 + 3 + 2 * k + n if n < 2 else 22)]

    def wait(self, place, sem):
        pltpu.make_async_remote_copy(
            src_ref=place,
            dst_ref=place,
            send_sem=self.send_sem,
            recv_sem=sem,
            device_id={"tp": self.at(0, 1)},
            device_id_type=MESH,
        ).wait_recv()

    def push(self, h, phase, k, first, second, part, direction):
        n = (0 if direction > 0 else 1) + (0 if part is None else 2)
        place = self.place(h, first, second, part)
        to = self.rel(h, direction, 0) if phase == 0 else self.rel(h, 0, direction)
        pltpu.make_async_remote_copy(
            src_ref=place,
            dst_ref=place,
            send_sem=self.send_sem,
            recv_sem=self.sem(h, phase, k, n),
            device_id={"tp": to},
            device_id_type=MESH,
        ).start()

    def both(self, h, phase, k, first):
        self.push(h, phase, k, first, 0, None, 1)
        self.push(h, phase, k, first, 0, None, -1)

    def relay(self, h, phase, k, n):
        off = (-1, 1)[n]
        first = OFFS[k] if phase else off
        second = off if phase else 0
        self.wait(self.place(h, first, second, None), self.sem(h, phase, k, n))
        self.push(h, phase, k, first, second, n, -off)

    def start(self):
        for h in (0, 1):
            self.both(h, 0, 0, 0)
        for h in (0, 1):
            self.both(h, 1, 0, 0)

    def run(self, step):
        if step == 0:
            self.start()
        elif step == 1:
            self.wait(self.buf.at[pl.ds(0, 4 * self.height)], self.sem(0, 1, 0, 2))
        elif step < 10:
            h = step - 2
            self.wait(self.place(h, 2, 0, None), self.sem(h, 0, 0, 2))
            self.both(h, 1, 3, 2)
        elif step < 20:
            h, n = (step - 10) // 2, step % 2
            self.relay(h, 0, 0, n)
            self.both(h, 1, n + 1, OFFS[n + 1])
        else:
            h, k, n = (step - 20) // 8, (step - 20) % 8 // 2, step % 2
            self.relay(h, 1, k, n)

    def finish(self):
        place = self.buf.at[pl.ds(0, (NTP - 1) * self.height)]
        pltpu.make_async_remote_copy(
            src_ref=place,
            dst_ref=place,
            send_sem=self.send_sem,
            recv_sem=self.sem(0, 1, 0, 2),
            device_id={"tp": self.at(0, 1)},
            device_id_type=MESH,
        ).wait_send()


class Exchange:
    def __init__(self, src, dst, send, recv, number, near):
        self.src, self.dst, self.near = src, dst, near
        self.send_sem, self.recv_sem = send.at[number], recv.at[number]
        self.me = lax.axis_index("ep")
        self.core = lax.rem(self.me, 2)
        self.rows = NEAR_SEND if near else HALF

    def block(self, ref, index):
        return ref.at[pl.ds(pl.multiple_of(index * self.rows, self.rows), self.rows)]

    def send(self, index, to, there):
        pltpu.make_async_remote_copy(
            src_ref=self.block(self.src, index),
            dst_ref=self.block(self.dst, there),
            send_sem=self.send_sem,
            recv_sem=self.recv_sem,
            device_id={"ep": to},
            device_id_type=MESH,
        ).start()

    def start(self):
        me, core = self.me, self.core
        if self.near:
            for j in (0, 1, 8, 9, 2, 3, 6, 7):
                self.send(j, lax.rem(me - core + (j - 4 + NEP), NEP), core + (8 - 2 * (j // 2)))
            self.send(5 - core, me + 1 - 2 * core, core + 4)
            own = pl.ds(pl.multiple_of((core + 4) * self.rows, self.rows), self.rows)
            self.dst[own, :] = self.src[own, :]
        else:
            for j in sorted(range(FAR), key=lambda j: abs(j // 2 - 5)):
                self.send(j, lax.rem(me - core + (j + 6), NEP), core + (20 - 2 * (j // 2)))

    def all_of(self):
        span = pl.ds(0, (NEAR - 1 if self.near else FAR) * self.rows)
        return pltpu.make_async_remote_copy(
            src_ref=self.src.at[span],
            dst_ref=self.dst.at[span],
            send_sem=self.send_sem,
            recv_sem=self.recv_sem,
            device_id={"ep": lax.rem(self.me + 1, NEP)},
            device_id_type=MESH,
        )

    def arrive(self):
        self.all_of().wait_recv()

    def finish(self):
        self.all_of().wait_send()


def iota(shape, dim):
    return lax.broadcasted_iota(jnp.int32, shape, dim)


def dot(a, b):
    return jnp.dot(a, b, preferred_element_type=F32)


def conv_span(ext, taps, cg, tp, channels, start, length):
    def group(g, carry):
        parts = []
        for u in range(2):
            rows = pl.ds(pl.multiple_of(g * 16, 16) + 8 * u, 8)
            wide = ext[rows, pl.ds(start - 128, length + 128)]
            tap = taps[rows, :]
            sums = [None] * 4
            for b in range(8):
                moved = pltpu.roll(wide, b, 1) if b else wide
                for a in range(4):
                    j = TAPS - 1 - (8 * a + b)
                    if j >= 0:
                        lane = jnp.broadcast_to(tap[:, j : j + 1], (8, 128))
                        term = jnp.concatenate([lane] * (length // 128 + 1), axis=1) * moved
                        sums[a] = term if sums[a] is None else sums[a] + term
            total = sums[0]
            for a in range(1, 4):
                total = total + pltpu.roll(sums[a], 8 * a, 1)
            parts.append(total[:, 128:])
        own = pl.ds(pl.multiple_of(tp * channels + g * 16, 16), 16)
        cg[own, :] = jnp.concatenate(parts, axis=0).astype(BF16)
        return carry

    lax.fori_loop(0, channels // 16, group, 0, unroll=UNROLL)


def kernel(
    value_hbm,
    gate_hbm,
    taps_hbm,
    gain_hbm,
    shift_hbm,
    rows_hbm,
    row_gain_hbm,
    ids_hbm,
    shares_hbm,
    ow_hbm,
    wg_hbm,
    wu_hbm,
    wd_hbm,
    mixed_ref,
    routed_ref,
    value_ref,
    gate_ref,
    taps_ref,
    gain_ref,
    shift_ref,
    rows_ref,
    row_gain_ref,
    ids_ref,
    shares_ref,
    ext,
    taps,
    tap_pad,
    tail,
    halo,
    cg_late,
    cg,
    out0,
    out1,
    outn,
    arr1,
    near,
    x0,
    x1,
    h0,
    h1,
    hn,
    y0,
    y1,
    yn,
    r0,
    r1,
    rn,
    mix,
    mixn,
    ow,
    wgu,
    wd,
    load_sem,
    send,
    recv,
    zsend,
    zrecv,
    halo_sem,
):
    ep, tp = lax.axis_index("ep"), lax.axis_index("tp")
    channels, length = value_hbm.shape
    count, width = rows_hbm.shape
    cols = width // NTP

    barrier = pltpu.get_barrier_semaphore()
    y, x = tp // NX, lax.rem(tp, NX)
    for dy, dx in ((0, 1), (0, 3), (1, 0), (3, 0)):
        to = lax.rem(y + dy, NY) * NX + lax.rem(x + dx, NX)
        pl.semaphore_signal(barrier, inc=1, device_id={"tp": to}, device_id_type=MESH)

    def greet(d, carry):
        pl.semaphore_signal(
            barrier, inc=1, device_id={"ep": lax.rem(ep + d, NEP)}, device_id_type=MESH
        )
        return carry

    lax.fori_loop(1, NEP, greet, 0)

    pairs = (
        (ids_hbm, ids_ref),
        (shares_hbm, shares_ref),
        (rows_hbm, rows_ref),
        (row_gain_hbm, row_gain_ref),
        (value_hbm, value_ref),
        (gate_hbm, gate_ref),
        (taps_hbm, taps_ref),
        (gain_hbm, gain_ref),
        (shift_hbm, shift_ref),
        (ow_hbm, ow),
        (wg_hbm.at[0], wgu.at[:, pl.ds(0, cols)]),
        (wu_hbm.at[0], wgu.at[:, pl.ds(cols, cols)]),
        (wd_hbm.at[0], wd),
    )
    loads = [pltpu.make_async_copy(a, b, load_sem.at[i]) for i, (a, b) in enumerate(pairs)]
    for load in loads:
        load.start()
    for load in loads[:2]:
        load.wait()

    expert = iota((NEP, count), 0)
    chosen = jnp.zeros((NEP, count), F32)
    share = jnp.zeros((NEP, count), F32)
    for k in range(ids_ref.shape[0]):
        here = ids_ref[k : k + 1, :] == expert
        chosen = jnp.where(here, 1.0, chosen)
        share = jnp.where(here, shares_ref[k : k + 1, :], share)
    earlier = (iota((count, count), 0) < iota((count, count), 1)).astype(F32).astype(BF16)
    place = jnp.where(chosen > 0.5, dot(chosen.astype(BF16), earlier), -1.0)
    place_b = place.astype(BF16)
    for load in loads[2:4]:
        load.wait()
    total = jnp.zeros((count, cols), F32)
    for t in range(NTP):
        total = total + rows_ref[:, t * cols : (t + 1) * cols].astype(F32)
    mean = jnp.sum(total, axis=1, keepdims=True) * (1.0 / width)
    total = jnp.zeros((count, cols), F32)
    for t in range(NTP):
        off = rows_ref[:, t * cols : (t + 1) * cols].astype(F32) - mean
        total = total + off * off
    var = jnp.sum(total, axis=1, keepdims=True) * (1.0 / width)
    mine = rows_ref[:, pl.ds(pl.multiple_of(tp * cols, cols), cols)].astype(F32)
    normed = ((mine - mean) * lax.rsqrt(var + 1e-05) * row_gain_ref[pl.ds(tp, 1), :]).astype(BF16)
    base = ep - lax.rem(ep, 2)

    def owners(shape, dim, bits, first):
        owner = jnp.bitwise_and(lax.shift_right_logical(iota(shape, dim), bits) + (base + first + NEP), NEP - 1)
        return (owner == iota(shape, 1 - dim)).astype(F32).astype(BF16)

    slot_of = dot(owners((FAR_ROWS, NEP), 0, 4, 6), place_b)
    slot = jnp.bitwise_and(iota((FAR_ROWS, count), 0), HALF - 1).astype(F32)
    for c, out in enumerate((out0, out1)):
        pick = (slot_of == slot + float(HALF * c)).astype(F32).astype(BF16)
        out[...] = dot(pick, normed).astype(BF16)

    def send_near():
        shape = (NEAR * NEAR_SEND, count)
        at = dot(owners((shape[0], NEP), 0, 5, -4), place_b)
        slot = jnp.bitwise_and(iota(shape, 0), NEAR_SEND - 1).astype(F32)
        pick = (at == slot).astype(F32).astype(BF16)
        scale = lax.rsqrt(var + 1e-05)
        for t in range(0, NTP, 2):
            parts = []
            for u in (t, t + 1):
                part = (rows_ref[:, u * cols : (u + 1) * cols].astype(F32) - mean) * scale
                parts.append((part * row_gain_ref[u : u + 1, :]).astype(BF16))
            pair = dot(pick, jnp.concatenate(parts, axis=1))
            outn[:, t * cols : (t + 2) * cols] = pair.astype(BF16)
        gon.start()

    for load in loads[4:7]:
        load.wait()
    gated = (value_ref[...].astype(F32) * sigmoid(gate_ref[...].astype(F32))).astype(BF16)
    tail[...] = gated[:, length - 128 :]
    ext[:, pl.ds(128, length)] = gated.astype(F32)
    tap_pad[pl.ds(0, TAPS), pl.ds(0, channels)] = taps_ref[...]
    taps[...] = tap_pad[...].T

    pl.semaphore_wait(barrier, 4 + NEP - 1)
    halo_copy = pltpu.make_async_remote_copy(
        src_ref=tail,
        dst_ref=halo,
        send_sem=halo_sem.at[0],
        recv_sem=halo_sem.at[1],
        device_id={"ep": lax.rem(ep + 1, NEP)},
        device_id_type=MESH,
    )
    halo_copy.start()
    own = pl.ds(pl.multiple_of(tp * FAR_ROWS, 16), FAR_ROWS)
    go0 = Exchange(out0, x0.at[own], zsend, zrecv, 0, False)
    go1 = Exchange(out1, arr1, zsend, zrecv, 1, False)
    gon = Exchange(outn, near, zsend, zrecv, 2, True)
    go0.start()
    go1.start()
    half = length // 2
    conv_span(ext, taps, cg, tp, channels, 128 + half, half)
    refs = ((cg, 1), (cg_late, 1), (x0, 0), (x1, 0), (h0, 0), (h1, 0), (hn, 0))
    gathers = [TpGather(ref, send, recv, i, axis) for i, (ref, axis) in enumerate(refs)]
    back0 = Exchange(y0, r0, zsend, zrecv, 3, False)
    back1 = Exchange(y1, r1, zsend, zrecv, 4, False)
    backn = Exchange(yn, rn, zsend, zrecv, 5, True)

    def conv_late():
        halo_copy.wait_recv()
        ext[:, pl.ds(0, 128)] = jnp.where(ep > 0, halo[...].astype(F32), 0.0)
        conv_span(ext, taps, cg_late, tp, channels, 128, half)

    def halves(n):
        first = (n // 16 + 1) // 2 * 16
        return (0, first), (first, n - first)

    def wide_rows(ref, start, size):
        n = ref.shape[0] // NTP
        return jnp.concatenate([ref[t * n + start : t * n + start + size, :] for t in range(NTP)], axis=1)

    def activate(lhs):
        pre = dot(lhs, wgu[...])
        g = jnp.minimum(pre[:, :cols], 7.0)
        u = jnp.clip(pre[:, cols:], -7.0, 7.0)
        return ((u + 1.0) * g * sigmoid(1.702 * g)).astype(BF16)

    def up(xs, hs):
        n = xs.shape[0] // NTP
        for start, size in halves(n):
            own = pl.ds(pl.multiple_of(tp * n + start, 16), size)
            hs[own, :] = activate(wide_rows(xs, start, size))

    def down(hs):
        parts = [dot(wide_rows(hs, *part), wd[...]).astype(BF16) for part in halves(hs.shape[0] // NTP)]
        return jnp.concatenate(parts, axis=0)

    def moved(shape, dim, block, room):
        row = iota(shape, dim).astype(F32)
        row = row + jnp.floor((row + 0.5) * (1.0 / block)) * float(room - block)
        return (row == iota(shape, 1 - dim).astype(F32)).astype(F32).astype(BF16)

    def compact():
        go1.arrive()
        own = pl.ds(pl.multiple_of(tp * LATE_ROWS, 16), LATE_ROWS)
        x1[own, :] = dot(moved((LATE_ROWS, FAR_ROWS), 0, OTHER, HALF), arr1[...]).astype(BF16)

    def up_near():
        gon.arrive()
        room = NEAR * NEAR_SEND
        act = [activate(near[i * room // 2 : (i + 1) * room // 2, :]) for i in range(2)]
        own = pl.ds(pl.multiple_of(tp * NEAR_ROWS, 16), NEAR_ROWS)
        turn_in = moved((NEAR_ROWS, room), 0, SLOTS, NEAR_SEND)
        hn[own, :] = dot(turn_in, jnp.concatenate(act, axis=0)).astype(BF16)

    def return_first():
        y0[...] = down(h0)
        back0.start()

    def return_second():
        y1[...] = dot(moved((FAR_ROWS, LATE_ROWS), 1, OTHER, HALF), down(h1)).astype(BF16)
        back1.start()

    def return_near():
        turn_out = moved((NEAR * NEAR_SEND, NEAR_ROWS), 1, SLOTS, NEAR_SEND)
        yn[...] = dot(turn_out, down(hn)).astype(BF16)
        backn.start()

    whole = NTP * channels
    groups = whole // 128
    stride = 256

    def project_ready():
        for load in loads[7:10]:
            load.wait()
        blank = jnp.zeros((16 - groups, 128), F32)
        gains = 0.5 * jnp.concatenate([gain_ref[...], blank], axis=0).T
        shifts = 0.5 * jnp.concatenate([shift_ref[...], blank], axis=0).T
        turned = jnp.concatenate([ow[i * 128 : (i + 1) * 128, :].T for i in range(groups)], axis=1)
        return gains, shifts, turned

    def project(buf, i, first, gains, shifts, turned):
        lanes = pl.ds(i * stride, stride)
        acc = jnp.zeros((128, stride), F32)
        for t in range(groups):
            acc = acc + buf[t * 128 : (t + 1) * 128, lanes].astype(F32)
        row_mean = jnp.sum(acc, axis=0, keepdims=True) * (1.0 / whole)
        acc = jnp.zeros((128, stride), F32)
        for t in range(groups):
            off = buf[t * 128 : (t + 1) * 128, lanes].astype(F32) - row_mean
            acc = acc + off * off
        row_var = jnp.sum(acc, axis=0, keepdims=True) * (1.0 / whole)
        scale = lax.rsqrt(row_var + 1e-05)
        for t in range(groups):
            v = (buf[t * 128 : (t + 1) * 128, lanes].astype(F32) - row_mean) * scale
            v = v * gains[:, t : t + 1] + shifts[:, t : t + 1]
            buf[t * 128 : (t + 1) * 128, lanes] = (v * jnp.tanh(v) + v).astype(BF16)
        mixed = dot(turned, buf[:, lanes])
        mixed_ref[pl.ds(first + i * stride, stride), :] = mixed.T.astype(BF16)

    def turn(a):
        eye = (iota((count, count), 0) == iota((count, count), 1)).astype(F32).astype(BF16)
        return lax.dot_general(eye, a, (((1,), (1,)), ((), ())), preferred_element_type=F32).astype(BF16)

    def prepare():
        share_hi = share.astype(BF16)
        share_lo = (share - share_hi.astype(F32)).astype(BF16)
        tables = [turn(a) for a in (place_b, share_hi, share_lo)]
        for columns, bits, first, out in ((FAR_ROWS, 4, 6, mix), (NEAR * NEAR_SEND, 5, -4, mixn)):
            widen = owners((NEP, columns), 1, bits, first)
            slot_at, hi_at, lo_at = [dot(a, widen) for a in tables]
            slot = jnp.bitwise_and(iota((count, columns), 1), (1 << bits) - 1).astype(F32)
            for c in range(out.shape[0] // 2):
                there = slot_at == slot + float(HALF * c)
                out[2 * c] = jnp.where(there, hi_at, 0.0).astype(BF16)
                out[2 * c + 1] = jnp.where(there, lo_at, 0.0).astype(BF16)

    def weigh(table, c, back, r):
        back.arrive()
        return dot(table[2 * c], r[...]) + dot(table[2 * c + 1], r[...])

    kept = {}

    def first_up():
        loads[10].wait()
        loads[11].wait()
        up(x0, h0)

    def first_down():
        loads[12].wait()
        return_first()

    def project_early():
        gathers[0].finish()
        kept[0] = project_ready()
        project(cg, 0, half, *kept[0])

    def project_late():
        gathers[1].finish()
        project(cg_late, 0, 0, *kept[0])

    def add(table, c, back, r):
        value = weigh(table, c, back, r)
        kept[1] = kept[1] + value if 1 in kept else value

    work = (
        conv_late,
        send_near,
        go0.arrive,
        compact,
        first_up,
        lambda: up(x1, h1),
        up_near,
        first_down,
        return_second,
        return_near,
        project_early,
        lambda: project(cg, 1, half, *kept[0]),
        project_late,
        lambda: project(cg_late, 1, 0, *kept[0]),
        prepare,
        lambda: add(mix, 0, back0, r0),
        lambda: add(mixn, 0, backn, rn),
        lambda: add(mix, 1, back1, r1),
    )
    for step in ORDER:
        if step < 900:
            gathers[step // 100].run(step % 100)
        else:
            work[step - 900]()
    routed_ref[...] = kept[1].astype(BF16)

    halo_copy.wait_send()
    for transfer in (go0, go1, gon, *gathers[2:], back0, back1, backn):
        transfer.finish()


def body(
    value_in,
    gate_in,
    conv_kernel,
    norm_gain,
    norm_shift,
    out_weight,
    expert_input,
    expert_gain,
    route_ids,
    route_weights,
    gate_weight,
    up_weight,
    down_weight,
):
    length, channels = value_in.shape
    count, width = expert_input.shape
    cols = width // NTP
    vmem = pl.BlockSpec(memory_space=pltpu.VMEM)
    hbm = pl.BlockSpec(memory_space=pltpu.HBM)
    mixed_out, routed_out = pl.pallas_call(
        kernel,
        out_shape=(
            pltpu.VMEM((length, out_weight.shape[1]), BF16),
            pltpu.VMEM((count, cols), BF16),
        ),
        in_specs=[hbm] * 13,
        out_specs=(vmem, vmem),
        scratch_shapes=[
            pltpu.VMEM((channels, length), BF16),
            pltpu.VMEM((channels, length), BF16),
            pltpu.VMEM(conv_kernel.shape, F32),
            pltpu.VMEM((NTP * channels // 128, 128), F32),
            pltpu.VMEM((NTP * channels // 128, 128), F32),
            pltpu.VMEM((count, width), BF16),
            pltpu.VMEM((NTP, cols), F32),
            pltpu.VMEM(route_ids.shape[::-1], jnp.int32),
            pltpu.VMEM(route_ids.shape[::-1], F32),
            pltpu.VMEM((channels, 128 + length), F32),
            pltpu.VMEM((128, 32), F32),
            pltpu.VMEM((32, 128), F32),
            pltpu.VMEM((channels, 128), BF16),
            pltpu.VMEM((channels, 128), BF16),
            pltpu.VMEM((NTP * channels, length // 2), BF16),
            pltpu.VMEM((NTP * channels, length // 2), BF16),
            pltpu.VMEM((FAR_ROWS, cols), BF16),
            pltpu.VMEM((FAR_ROWS, cols), BF16),
            pltpu.VMEM((NEAR * NEAR_SEND, width), BF16),
            pltpu.VMEM((FAR_ROWS, cols), BF16),
            pltpu.VMEM((NEAR * NEAR_SEND, width), BF16),
            pltpu.VMEM((NTP * FAR_ROWS, cols), BF16),
            pltpu.VMEM((NTP * LATE_ROWS, cols), BF16),
            pltpu.VMEM((NTP * FAR_ROWS, cols), BF16),
            pltpu.VMEM((NTP * LATE_ROWS, cols), BF16),
            pltpu.VMEM((NTP * NEAR_ROWS, cols), BF16),
            pltpu.VMEM((FAR_ROWS, cols), BF16),
            pltpu.VMEM((FAR_ROWS, cols), BF16),
            pltpu.VMEM((NEAR * NEAR_SEND, cols), BF16),
            pltpu.VMEM((FAR_ROWS, cols), BF16),
            pltpu.VMEM((FAR_ROWS, cols), BF16),
            pltpu.VMEM((NEAR * NEAR_SEND, cols), BF16),
            pltpu.VMEM((4, count, FAR_ROWS), BF16),
            pltpu.VMEM((2, count, NEAR * NEAR_SEND), BF16),
            pltpu.VMEM(out_weight.shape, BF16),
            pltpu.VMEM((width, 2 * cols), BF16),
            pltpu.VMEM((width, cols), BF16),
            pltpu.SemaphoreType.DMA((13,)),
            pltpu.SemaphoreType.DMA((7,)),
            pltpu.SemaphoreType.DMA((7 * 23,)),
            pltpu.SemaphoreType.DMA((6,)),
            pltpu.SemaphoreType.DMA((6,)),
            pltpu.SemaphoreType.DMA((2,)),
        ],
        compiler_params=pltpu.CompilerParams(
            collective_id=0, has_side_effects=True, vmem_limit_bytes=60 * 1024 * 1024
        ),
        name="whole",
    )(
        value_in.T,
        gate_in.T,
        conv_kernel,
        norm_gain.reshape(-1, 128),
        norm_shift.reshape(-1, 128),
        expert_input,
        expert_gain.reshape(NTP, cols),
        route_ids.T,
        route_weights.T,
        out_weight,
        gate_weight,
        up_weight,
        down_weight,
    )
    return (mixed_out, routed_out)


def solution(mesh):
    return jax.shard_map(
        body,
        mesh=mesh,
        in_specs=(
            P("ep", "tp"),
            P("ep", "tp"),
            P(None, "tp"),
            P(),
            P(),
            P(None, "tp"),
            P("ep", None),
            P(),
            P("ep", None),
            P("ep", None),
            P("ep", None, "tp"),
            P("ep", None, "tp"),
            P("ep", None, "tp"),
        ),
        out_specs=(P("ep", "tp"), P("ep", "tp")),
        check_vma=False,
    )
```

```python
import jax
import jax.numpy as jnp
from jax import lax
from jax.experimental import pallas as pl
from jax.experimental.pallas import tpu as pltpu
from jax.sharding import PartitionSpec as P

MESH = pl.DeviceIdType.MESH
F32, BF16 = jnp.float32, jnp.bfloat16
NX = 4
NY = 4
NTP = NX * NY
NEP = 32
HALF = 16
OTHER = 14
SLOTS = HALF + OTHER
NEAR = 10
FAR = 22
FAR_ROWS = FAR * HALF
LATE_ROWS = 320
NEAR_SEND = 32
NEAR_ROWS = 304
TAPS = 31
UNROLL = 6
OFFS = (0, -1, 1, 2)

ORDER = (
    0, 900, 10, 20, 2, 21, 22, 901, 902, 200, 23, 210, 903, 300, 220, 1,
    910, 911, 202, 221, 222, 310, 320, 223, 302, 321, 322, 914, 201, 904, 400, 323,
    906, 410, 420, 301, 905, 500, 402, 421, 422, 510, 600, 520, 423, 502, 521, 522,
    610, 620, 401, 907, 523, 100, 602, 621, 622, 501, 908, 110, 120, 623, 102, 121,
    122, 601, 909, 123, 915, 101, 912, 913, 916, 917,
)


def sigmoid(v):
    return 0.5 * jnp.tanh(0.5 * v) + 0.5


class TpGather:
    def __init__(self, buf, send, recv, number, axis):
        self.buf, self.axis = buf, axis
        self.height = buf.shape[0] // NTP
        self.size = self.height if axis == 0 else buf.shape[1]
        self.send_sem, self.recv_sem, self.base = send.at[number], recv, number * 7
        unit = 16 if axis == 0 else 128
        whole = self.size // unit
        self.spans = {}
        for h, (at, size) in enumerate(((0, (whole + 1) // 2), ((whole + 1) // 2, whole // 2))):
            first = (size + 1) // 2
            self.spans[h, None] = (at * unit, size * unit)
            self.spans[h, 0] = (at * unit, first * unit)
            self.spans[h, 1] = ((at + first) * unit, (size - first) * unit)
        tp = lax.axis_index("tp")
        self.y, self.x = tp // NX, lax.rem(tp, NX)

    def at(self, dy, dx):
        return lax.rem(self.y + (dy + NY), NY) * NX + lax.rem(self.x + (dx + NX), NX)

    def rel(self, h, first, second):
        return self.at(second, first) if h == 0 else self.at(first, second)

    def place(self, h, first, second, part):
        start, size = self.spans[h, part]
        row = self.rel(h, first, second) * self.height
        if self.axis == 0:
            return self.buf.at[pl.ds(pl.multiple_of(row + start, 16), size)]
        return self.buf.at[pl.ds(pl.multiple_of(row, 16), self.height), pl.ds(start, size)]

    def sem(self, h, phase, k, n):
        if phase == 0:
            return self.recv_sem.at[self.base + n // 2]
        return self.recv_sem.at[self.base + (2 + k if n < 2 else 6)]

    def wait(self, place, sem):
        pltpu.make_async_remote_copy(
            src_ref=place,
            dst_ref=place,
            send_sem=self.send_sem,
            recv_sem=sem,
            device_id={"tp": self.at(0, 1)},
            device_id_type=MESH,
        ).wait_recv()

    def push(self, h, phase, k, first, second, part, direction):
        n = (0 if direction > 0 else 1) + (0 if part is None else 2)
        place = self.place(h, first, second, part)
        to = self.rel(h, direction, 0) if phase == 0 else self.rel(h, 0, direction)
        pltpu.make_async_remote_copy(
            src_ref=place,
            dst_ref=place,
            send_sem=self.send_sem,
            recv_sem=self.sem(h, phase, k, n),
            device_id={"tp": to},
            device_id_type=MESH,
        ).start()

    def both(self, h, phase, k, first):
        self.push(h, phase, k, first, 0, None, 1)
        self.push(h, phase, k, first, 0, None, -1)

    def pass_on(self, h, phase, k, n):
        off = (-1, 1)[n]
        first = OFFS[k] if phase else off
        second = off if phase else 0
        self.push(h, phase, k, first, second, n, -off)

    def start(self):
        for h in (0, 1):
            self.both(h, 0, 0, 0)
        for h in (0, 1):
            self.both(h, 1, 0, 0)

    def run(self, step):
        if step == 0:
            self.start()
            return
        shards = 4 if step == 1 else 1 if step == 2 else 2
        phase = 0 if step in (2, 10) else 1
        k = step - 20 if step >= 20 else 0
        self.wait(self.buf.at[pl.ds(0, shards * self.height)], self.sem(0, phase, k, 2 if step < 10 else 0))
        for h in (0, 1):
            if step == 2:
                self.both(h, 1, 3, 2)
            elif step == 10:
                for n in (0, 1):
                    self.pass_on(h, 0, 0, n)
            elif step >= 20:
                for n in (0, 1):
                    self.pass_on(h, 1, k, n)
        if step == 10:
            for n in (0, 1):
                for h in (0, 1):
                    self.both(h, 1, n + 1, OFFS[n + 1])

    def finish(self):
        place = self.buf.at[pl.ds(0, (NTP - 1) * self.height)]
        pltpu.make_async_remote_copy(
            src_ref=place,
            dst_ref=place,
            send_sem=self.send_sem,
            recv_sem=self.sem(0, 1, 0, 2),
            device_id={"tp": self.at(0, 1)},
            device_id_type=MESH,
        ).wait_send()


class Exchange:
    def __init__(self, src, dst, send, recv, number, near):
        self.src, self.dst, self.near = src, dst, near
        self.send_sem, self.recv_sem = send.at[number], recv.at[number]
        self.me = lax.axis_index("ep")
        self.core = lax.rem(self.me, 2)
        self.rows = NEAR_SEND if near else HALF

    def block(self, ref, index):
        return ref.at[pl.ds(pl.multiple_of(index * self.rows, self.rows), self.rows)]

    def send(self, index, to, there):
        pltpu.make_async_remote_copy(
            src_ref=self.block(self.src, index),
            dst_ref=self.block(self.dst, there),
            send_sem=self.send_sem,
            recv_sem=self.recv_sem,
            device_id={"ep": to},
            device_id_type=MESH,
        ).start()

    def start(self):
        me, core = self.me, self.core
        if self.near:
            for j in (0, 1, 8, 9, 2, 3, 6, 7):
                self.send(j, lax.rem(me - core + (j - 4 + NEP), NEP), core + (8 - 2 * (j // 2)))
            self.send(5 - core, me + 1 - 2 * core, core + 4)
            own = pl.ds(pl.multiple_of((core + 4) * self.rows, self.rows), self.rows)
            self.dst[own, :] = self.src[own, :]
        else:
            for j in sorted(range(FAR), key=lambda j: abs(j // 2 - 5)):
                self.send(j, lax.rem(me - core + (j + 6), NEP), core + (20 - 2 * (j // 2)))

    def all_of(self):
        span = pl.ds(0, (NEAR - 1 if self.near else FAR) * self.rows)
        return pltpu.make_async_remote_copy(
            src_ref=self.src.at[span],
            dst_ref=self.dst.at[span],
            send_sem=self.send_sem,
            recv_sem=self.recv_sem,
            device_id={"ep": lax.rem(self.me + 1, NEP)},
            device_id_type=MESH,
        )

    def arrive(self):
        self.all_of().wait_recv()

    def finish(self):
        self.all_of().wait_send()


def iota(shape, dim):
    return lax.broadcasted_iota(jnp.int32, shape, dim)


def dot(a, b):
    return jnp.dot(a, b, preferred_element_type=F32)


def conv_span(ext, taps, cg, tp, channels, start, length):
    def group(g, carry):
        parts = []
        for u in range(2):
            rows = pl.ds(pl.multiple_of(g * 16, 16) + 8 * u, 8)
            wide = ext[rows, pl.ds(start - 128, length + 128)]
            tap = taps[rows, :]
            sums = [None] * 4
            for b in range(8):
                moved = pltpu.roll(wide, b, 1) if b else wide
                for a in range(4):
                    j = TAPS - 1 - (8 * a + b)
                    if j >= 0:
                        lane = jnp.broadcast_to(tap[:, j : j + 1], (8, 128))
                        term = jnp.concatenate([lane] * (length // 128 + 1), axis=1) * moved
                        sums[a] = term if sums[a] is None else sums[a] + term
            total = sums[0]
            for a in range(1, 4):
                total = total + pltpu.roll(sums[a], 8 * a, 1)
            parts.append(total[:, 128:])
        own = pl.ds(pl.multiple_of(tp * channels + g * 16, 16), 16)
        cg[own, :] = jnp.concatenate(parts, axis=0).astype(BF16)
        return carry

    lax.fori_loop(0, channels // 16, group, 0, unroll=UNROLL)


def kernel(
    value_hbm,
    gate_hbm,
    taps_hbm,
    gain_hbm,
    shift_hbm,
    rows_hbm,
    row_gain_hbm,
    ids_hbm,
    shares_hbm,
    ow_hbm,
    wg_hbm,
    wu_hbm,
    wd_hbm,
    mixed_ref,
    routed_ref,
    value_ref,
    gate_ref,
    taps_ref,
    gain_ref,
    shift_ref,
    rows_ref,
    row_gain_ref,
    ids_ref,
    shares_ref,
    ext,
    taps,
    tap_pad,
    tail,
    halo,
    cg_late,
    cg,
    out0,
    out1,
    outn,
    arr1,
    near,
    x0,
    x1,
    h0,
    h1,
    hn,
    y0,
    y1,
    yn,
    r0,
    r1,
    rn,
    mix,
    mixn,
    ow,
    wgu,
    wd,
    load_sem,
    send,
    recv,
    zsend,
    zrecv,
    halo_sem,
):
    ep, tp = lax.axis_index("ep"), lax.axis_index("tp")
    channels, length = value_hbm.shape
    count, width = rows_hbm.shape
    cols = width // NTP

    barrier = pltpu.get_barrier_semaphore()
    y, x = tp // NX, lax.rem(tp, NX)
    for dy, dx in ((0, 1), (0, 3), (1, 0), (3, 0)):
        to = lax.rem(y + dy, NY) * NX + lax.rem(x + dx, NX)
        pl.semaphore_signal(barrier, inc=1, device_id={"tp": to}, device_id_type=MESH)

    def greet(d, carry):
        pl.semaphore_signal(
            barrier, inc=1, device_id={"ep": lax.rem(ep + d, NEP)}, device_id_type=MESH
        )
        return carry

    lax.fori_loop(1, NEP, greet, 0)

    pairs = (
        (ids_hbm, ids_ref),
        (shares_hbm, shares_ref),
        (rows_hbm, rows_ref),
        (row_gain_hbm, row_gain_ref),
        (value_hbm, value_ref),
        (gate_hbm, gate_ref),
        (taps_hbm, taps_ref),
        (gain_hbm, gain_ref),
        (shift_hbm, shift_ref),
        (ow_hbm, ow),
        (wg_hbm.at[0], wgu.at[:, pl.ds(0, cols)]),
        (wu_hbm.at[0], wgu.at[:, pl.ds(cols, cols)]),
        (wd_hbm.at[0], wd),
    )
    loads = [pltpu.make_async_copy(a, b, load_sem.at[i]) for i, (a, b) in enumerate(pairs)]
    for load in loads:
        load.start()
    for load in loads[:2]:
        load.wait()

    expert = iota((NEP, count), 0)
    chosen = jnp.zeros((NEP, count), F32)
    share = jnp.zeros((NEP, count), F32)
    for k in range(ids_ref.shape[0]):
        here = ids_ref[k : k + 1, :] == expert
        chosen = jnp.where(here, 1.0, chosen)
        share = jnp.where(here, shares_ref[k : k + 1, :], share)
    earlier = (iota((count, count), 0) < iota((count, count), 1)).astype(F32).astype(BF16)
    place = jnp.where(chosen > 0.5, dot(chosen.astype(BF16), earlier), -1.0)
    place_b = place.astype(BF16)
    for load in loads[2:4]:
        load.wait()
    total = jnp.zeros((count, cols), F32)
    for t in range(NTP):
        total = total + rows_ref[:, t * cols : (t + 1) * cols].astype(F32)
    mean = jnp.sum(total, axis=1, keepdims=True) * (1.0 / width)
    total = jnp.zeros((count, cols), F32)
    for t in range(NTP):
        off = rows_ref[:, t * cols : (t + 1) * cols].astype(F32) - mean
        total = total + off * off
    var = jnp.sum(total, axis=1, keepdims=True) * (1.0 / width)
    mine = rows_ref[:, pl.ds(pl.multiple_of(tp * cols, cols), cols)].astype(F32)
    normed = ((mine - mean) * lax.rsqrt(var + 1e-05) * row_gain_ref[pl.ds(tp, 1), :]).astype(BF16)
    base = ep - lax.rem(ep, 2)

    def owners(shape, dim, bits, first):
        owner = jnp.bitwise_and(lax.shift_right_logical(iota(shape, dim), bits) + (base + first + NEP), NEP - 1)
        return (owner == iota(shape, 1 - dim)).astype(F32).astype(BF16)

    slot_of = dot(owners((FAR_ROWS, NEP), 0, 4, 6), place_b)
    slot = jnp.bitwise_and(iota((FAR_ROWS, count), 0), HALF - 1).astype(F32)
    for c, out in enumerate((out0, out1)):
        pick = (slot_of == slot + float(HALF * c)).astype(F32).astype(BF16)
        out[...] = dot(pick, normed).astype(BF16)

    def send_near():
        shape = (NEAR * NEAR_SEND, count)
        at = dot(owners((shape[0], NEP), 0, 5, -4), place_b)
        slot = jnp.bitwise_and(iota(shape, 0), NEAR_SEND - 1).astype(F32)
        pick = (at == slot).astype(F32).astype(BF16)
        scale = lax.rsqrt(var + 1e-05)
        for t in range(0, NTP, 2):
            parts = []
            for u in (t, t + 1):
                part = (rows_ref[:, u * cols : (u + 1) * cols].astype(F32) - mean) * scale
                parts.append((part * row_gain_ref[u : u + 1, :]).astype(BF16))
            pair = dot(pick, jnp.concatenate(parts, axis=1))
            outn[:, t * cols : (t + 2) * cols] = pair.astype(BF16)
        gon.start()

    for load in loads[4:7]:
        load.wait()
    gated = (value_ref[...].astype(F32) * sigmoid(gate_ref[...].astype(F32))).astype(BF16)
    tail[...] = gated[:, length - 128 :]
    ext[:, pl.ds(128, length)] = gated.astype(F32)
    tap_pad[pl.ds(0, TAPS), pl.ds(0, channels)] = taps_ref[...]
    taps[...] = tap_pad[...].T

    pl.semaphore_wait(barrier, 4 + NEP - 1)
    halo_copy = pltpu.make_async_remote_copy(
        src_ref=tail,
        dst_ref=halo,
        send_sem=halo_sem.at[0],
        recv_sem=halo_sem.at[1],
        device_id={"ep": lax.rem(ep + 1, NEP)},
        device_id_type=MESH,
    )
    halo_copy.start()
    own = pl.ds(pl.multiple_of(tp * FAR_ROWS, 16), FAR_ROWS)
    go0 = Exchange(out0, x0.at[own], zsend, zrecv, 0, False)
    go1 = Exchange(out1, arr1, zsend, zrecv, 1, False)
    gon = Exchange(outn, near, zsend, zrecv, 2, True)
    go0.start()
    go1.start()
    half = length // 2
    conv_span(ext, taps, cg, tp, channels, 128 + half, half)
    refs = ((cg, 1), (cg_late, 1), (x0, 0), (x1, 0), (h0, 0), (h1, 0), (hn, 0))
    gathers = [TpGather(ref, send, recv, i, axis) for i, (ref, axis) in enumerate(refs)]
    back0 = Exchange(y0, r0, zsend, zrecv, 3, False)
    back1 = Exchange(y1, r1, zsend, zrecv, 4, False)
    backn = Exchange(yn, rn, zsend, zrecv, 5, True)

    def conv_late():
        halo_copy.wait_recv()
        ext[:, pl.ds(0, 128)] = jnp.where(ep > 0, halo[...].astype(F32), 0.0)
        conv_span(ext, taps, cg_late, tp, channels, 128, half)

    def halves(n):
        first = (n // 16 + 1) // 2 * 16
        return (0, first), (first, n - first)

    def wide_rows(ref, start, size):
        n = ref.shape[0] // NTP
        return jnp.concatenate([ref[t * n + start : t * n + start + size, :] for t in range(NTP)], axis=1)

    def activate(lhs):
        pre = dot(lhs, wgu[...])
        g = jnp.minimum(pre[:, :cols], 7.0)
        u = jnp.clip(pre[:, cols:], -7.0, 7.0)
        return ((u + 1.0) * g * sigmoid(1.702 * g)).astype(BF16)

    def up(xs, hs):
        n = xs.shape[0] // NTP
        for start, size in halves(n):
            own = pl.ds(pl.multiple_of(tp * n + start, 16), size)
            hs[own, :] = activate(wide_rows(xs, start, size))

    def down(hs):
        parts = [dot(wide_rows(hs, *part), wd[...]).astype(BF16) for part in halves(hs.shape[0] // NTP)]
        return jnp.concatenate(parts, axis=0)

    def moved(shape, dim, block, room):
        row = iota(shape, dim).astype(F32)
        row = row + jnp.floor((row + 0.5) * (1.0 / block)) * float(room - block)
        return (row == iota(shape, 1 - dim).astype(F32)).astype(F32).astype(BF16)

    def compact():
        go1.arrive()
        own = pl.ds(pl.multiple_of(tp * LATE_ROWS, 16), LATE_ROWS)
        x1[own, :] = dot(moved((LATE_ROWS, FAR_ROWS), 0, OTHER, HALF), arr1[...]).astype(BF16)

    def up_near():
        gon.arrive()
        room = NEAR * NEAR_SEND
        act = [activate(near[i * room // 2 : (i + 1) * room // 2, :]) for i in range(2)]
        own = pl.ds(pl.multiple_of(tp * NEAR_ROWS, 16), NEAR_ROWS)
        turn_in = moved((NEAR_ROWS, room), 0, SLOTS, NEAR_SEND)
        hn[own, :] = dot(turn_in, jnp.concatenate(act, axis=0)).astype(BF16)

    def return_first():
        y0[...] = down(h0)
        back0.start()

    def return_second():
        y1[...] = dot(moved((FAR_ROWS, LATE_ROWS), 1, OTHER, HALF), down(h1)).astype(BF16)
        back1.start()

    def return_near():
        turn_out = moved((NEAR * NEAR_SEND, NEAR_ROWS), 1, SLOTS, NEAR_SEND)
        yn[...] = dot(turn_out, down(hn)).astype(BF16)
        backn.start()

    whole = NTP * channels
    groups = whole // 128
    stride = 256

    def project_ready():
        for load in loads[7:10]:
            load.wait()
        blank = jnp.zeros((16 - groups, 128), F32)
        gains = 0.5 * jnp.concatenate([gain_ref[...], blank], axis=0).T
        shifts = 0.5 * jnp.concatenate([shift_ref[...], blank], axis=0).T
        turned = jnp.concatenate([ow[i * 128 : (i + 1) * 128, :].T for i in range(groups)], axis=1)
        return gains, shifts, turned

    def project(buf, i, first, gains, shifts, turned):
        lanes = pl.ds(i * stride, stride)
        acc = jnp.zeros((128, stride), F32)
        for t in range(groups):
            acc = acc + buf[t * 128 : (t + 1) * 128, lanes].astype(F32)
        row_mean = jnp.sum(acc, axis=0, keepdims=True) * (1.0 / whole)
        acc = jnp.zeros((128, stride), F32)
        for t in range(groups):
            off = buf[t * 128 : (t + 1) * 128, lanes].astype(F32) - row_mean
            acc = acc + off * off
        row_var = jnp.sum(acc, axis=0, keepdims=True) * (1.0 / whole)
        scale = lax.rsqrt(row_var + 1e-05)
        for t in range(groups):
            v = (buf[t * 128 : (t + 1) * 128, lanes].astype(F32) - row_mean) * scale
            v = v * gains[:, t : t + 1] + shifts[:, t : t + 1]
            buf[t * 128 : (t + 1) * 128, lanes] = (v * jnp.tanh(v) + v).astype(BF16)
        mixed = dot(turned, buf[:, lanes])
        mixed_ref[pl.ds(first + i * stride, stride), :] = mixed.T.astype(BF16)

    def turn(a):
        eye = (iota((count, count), 0) == iota((count, count), 1)).astype(F32).astype(BF16)
        return lax.dot_general(eye, a, (((1,), (1,)), ((), ())), preferred_element_type=F32).astype(BF16)

    def prepare():
        share_hi = share.astype(BF16)
        share_lo = (share - share_hi.astype(F32)).astype(BF16)
        tables = [turn(a) for a in (place_b, share_hi, share_lo)]
        for columns, bits, first, out in ((FAR_ROWS, 4, 6, mix), (NEAR * NEAR_SEND, 5, -4, mixn)):
            widen = owners((NEP, columns), 1, bits, first)
            slot_at, hi_at, lo_at = [dot(a, widen) for a in tables]
            slot = jnp.bitwise_and(iota((count, columns), 1), (1 << bits) - 1).astype(F32)
            for c in range(out.shape[0] // 2):
                there = slot_at == slot + float(HALF * c)
                out[2 * c] = jnp.where(there, hi_at, 0.0).astype(BF16)
                out[2 * c + 1] = jnp.where(there, lo_at, 0.0).astype(BF16)

    def weigh(table, c, back, r):
        back.arrive()
        return dot(table[2 * c], r[...]) + dot(table[2 * c + 1], r[...])

    kept = {}

    def first_up():
        loads[10].wait()
        loads[11].wait()
        up(x0, h0)

    def first_down():
        loads[12].wait()
        return_first()

    def project_early():
        gathers[0].finish()
        kept[0] = project_ready()
        project(cg, 0, half, *kept[0])

    def project_late():
        gathers[1].finish()
        project(cg_late, 0, 0, *kept[0])

    def add(table, c, back, r):
        value = weigh(table, c, back, r)
        kept[1] = kept[1] + value if 1 in kept else value

    work = (
        conv_late,
        send_near,
        go0.arrive,
        compact,
        first_up,
        lambda: up(x1, h1),
        up_near,
        first_down,
        return_second,
        return_near,
        project_early,
        lambda: project(cg, 1, half, *kept[0]),
        project_late,
        lambda: project(cg_late, 1, 0, *kept[0]),
        prepare,
        lambda: add(mix, 0, back0, r0),
        lambda: add(mixn, 0, backn, rn),
        lambda: add(mix, 1, back1, r1),
    )
    for step in ORDER:
        if step < 900:
            gathers[step // 100].run(step % 100)
        else:
            work[step - 900]()
    routed_ref[...] = kept[1].astype(BF16)

    halo_copy.wait_send()
    for transfer in (go0, go1, gon, *gathers[2:], back0, back1, backn):
        transfer.finish()


def body(
    value_in,
    gate_in,
    conv_kernel,
    norm_gain,
    norm_shift,
    out_weight,
    expert_input,
    expert_gain,
    route_ids,
    route_weights,
    gate_weight,
    up_weight,
    down_weight,
):
    length, channels = value_in.shape
    count, width = expert_input.shape
    cols = width // NTP
    vmem = pl.BlockSpec(memory_space=pltpu.VMEM)
    hbm = pl.BlockSpec(memory_space=pltpu.HBM)
    mixed_out, routed_out = pl.pallas_call(
        kernel,
        out_shape=(
            pltpu.VMEM((length, out_weight.shape[1]), BF16),
            pltpu.VMEM((count, cols), BF16),
        ),
        in_specs=[hbm] * 13,
        out_specs=(vmem, vmem),
        scratch_shapes=[
            pltpu.VMEM((channels, length), BF16),
            pltpu.VMEM((channels, length), BF16),
            pltpu.VMEM(conv_kernel.shape, F32),
            pltpu.VMEM((NTP * channels // 128, 128), F32),
            pltpu.VMEM((NTP * channels // 128, 128), F32),
            pltpu.VMEM((count, width), BF16),
            pltpu.VMEM((NTP, cols), F32),
            pltpu.VMEM(route_ids.shape[::-1], jnp.int32),
            pltpu.VMEM(route_ids.shape[::-1], F32),
            pltpu.VMEM((channels, 128 + length), F32),
            pltpu.VMEM((128, 32), F32),
            pltpu.VMEM((32, 128), F32),
            pltpu.VMEM((channels, 128), BF16),
            pltpu.VMEM((channels, 128), BF16),
            pltpu.VMEM((NTP * channels, length // 2), BF16),
            pltpu.VMEM((NTP * channels, length // 2), BF16),
            pltpu.VMEM((FAR_ROWS, cols), BF16),
            pltpu.VMEM((FAR_ROWS, cols), BF16),
            pltpu.VMEM((NEAR * NEAR_SEND, width), BF16),
            pltpu.VMEM((FAR_ROWS, cols), BF16),
            pltpu.VMEM((NEAR * NEAR_SEND, width), BF16),
            pltpu.VMEM((NTP * FAR_ROWS, cols), BF16),
            pltpu.VMEM((NTP * LATE_ROWS, cols), BF16),
            pltpu.VMEM((NTP * FAR_ROWS, cols), BF16),
            pltpu.VMEM((NTP * LATE_ROWS, cols), BF16),
            pltpu.VMEM((NTP * NEAR_ROWS, cols), BF16),
            pltpu.VMEM((FAR_ROWS, cols), BF16),
            pltpu.VMEM((FAR_ROWS, cols), BF16),
            pltpu.VMEM((NEAR * NEAR_SEND, cols), BF16),
            pltpu.VMEM((FAR_ROWS, cols), BF16),
            pltpu.VMEM((FAR_ROWS, cols), BF16),
            pltpu.VMEM((NEAR * NEAR_SEND, cols), BF16),
            pltpu.VMEM((4, count, FAR_ROWS), BF16),
            pltpu.VMEM((2, count, NEAR * NEAR_SEND), BF16),
            pltpu.VMEM(out_weight.shape, BF16),
            pltpu.VMEM((width, 2 * cols), BF16),
            pltpu.VMEM((width, cols), BF16),
            pltpu.SemaphoreType.DMA((13,)),
            pltpu.SemaphoreType.DMA((7,)),
            pltpu.SemaphoreType.DMA((7 * 7,)),
            pltpu.SemaphoreType.DMA((6,)),
            pltpu.SemaphoreType.DMA((6,)),
            pltpu.SemaphoreType.DMA((2,)),
        ],
        compiler_params=pltpu.CompilerParams(
            collective_id=0, has_side_effects=True, vmem_limit_bytes=60 * 1024 * 1024
        ),
        name="whole",
    )(
        value_in.T,
        gate_in.T,
        conv_kernel,
        norm_gain.reshape(-1, 128),
        norm_shift.reshape(-1, 128),
        expert_input,
        expert_gain.reshape(NTP, cols),
        route_ids.T,
        route_weights.T,
        out_weight,
        gate_weight,
        up_weight,
        down_weight,
    )
    return (mixed_out, routed_out)


def solution(mesh):
    return jax.shard_map(
        body,
        mesh=mesh,
        in_specs=(
            P("ep", "tp"),
            P("ep", "tp"),
            P(None, "tp"),
            P(),
            P(),
            P(None, "tp"),
            P("ep", None),
            P(),
            P("ep", None),
            P("ep", None),
            P("ep", None, "tp"),
            P("ep", None, "tp"),
            P("ep", None, "tp"),
        ),
        out_specs=(P("ep", "tp"), P("ep", "tp")),
        check_vma=False,
    )
```

```python
import jax
import jax.numpy as jnp
from jax import lax
from jax.experimental import pallas as pl
from jax.experimental.pallas import tpu as pltpu
from jax.sharding import PartitionSpec as P

MESH = pl.DeviceIdType.MESH
F32, BF16 = jnp.float32, jnp.bfloat16
NX = 4
NY = 4
NTP = NX * NY
NEP = 32
HALF = 16
OTHER = 14
SLOTS = HALF + OTHER
NEAR = 10
FAR = 22
FAR_ROWS = FAR * HALF
LATE_ROWS = 320
NEAR_SEND = 32
NEAR_ROWS = 304
TAPS = 31
UNROLL = 6
OFFS = (0, -1, 1, 2)

ORDER = (
    0, 900, 10, 20, 2, 21, 22, 901, 902, 200, 23, 210, 903, 300, 220, 1,
    910, 911, 202, 221, 222, 310, 320, 223, 302, 321, 322, 914, 201, 904, 400, 323,
    906, 410, 420, 301, 905, 500, 402, 421, 422, 510, 600, 520, 423, 502, 521, 522,
    610, 620, 401, 907, 523, 100, 602, 621, 622, 501, 908, 110, 120, 623, 102, 121,
    122, 601, 909, 123, 915, 101, 912, 913, 916, 917,
)


def sigmoid(v):
    return 0.5 * jnp.tanh(0.5 * v) + 0.5


class TpGather:
    def __init__(self, buf, send, recv, number, axis):
        self.buf, self.axis = buf, axis
        self.height = buf.shape[0] // NTP
        self.size = self.height if axis == 0 else buf.shape[1]
        self.send_sem, self.recv_sem, self.base = send.at[number], recv, number * 7
        unit = 16 if axis == 0 else 128
        whole = self.size // unit
        self.spans = {}
        for h, (at, size) in enumerate(((0, (whole + 1) // 2), ((whole + 1) // 2, whole // 2))):
            first = (size + 1) // 2
            self.spans[h, None] = (at * unit, size * unit)
            self.spans[h, 0] = (at * unit, first * unit)
            self.spans[h, 1] = ((at + first) * unit, (size - first) * unit)
        tp = lax.axis_index("tp")
        self.y, self.x = tp // NX, lax.rem(tp, NX)

    def at(self, dy, dx):
        return lax.rem(self.y + (dy + NY), NY) * NX + lax.rem(self.x + (dx + NX), NX)

    def rel(self, h, first, second):
        return self.at(second, first) if h == 0 else self.at(first, second)

    def place(self, h, first, second, part):
        start, size = self.spans[h, part]
        row = self.rel(h, first, second) * self.height
        if self.axis == 0:
            return self.buf.at[pl.ds(pl.multiple_of(row + start, 16), size)]
        return self.buf.at[pl.ds(pl.multiple_of(row, 16), self.height), pl.ds(start, size)]

    def sem(self, h, phase, k, n):
        if phase == 0:
            return self.recv_sem.at[self.base + n // 2]
        return self.recv_sem.at[self.base + (2 + k if n < 2 else 6)]

    def wait(self, place, sem):
        pltpu.make_async_remote_copy(
            src_ref=place,
            dst_ref=place,
            send_sem=self.send_sem,
            recv_sem=sem,
            device_id={"tp": self.at(0, 1)},
            device_id_type=MESH,
        ).wait_recv()

    def push(self, h, phase, k, first, second, part, direction):
        n = (0 if direction > 0 else 1) + (0 if part is None else 2)
        place = self.place(h, first, second, part)
        to = self.rel(h, direction, 0) if phase == 0 else self.rel(h, 0, direction)
        pltpu.make_async_remote_copy(
            src_ref=place,
            dst_ref=place,
            send_sem=self.send_sem,
            recv_sem=self.sem(h, phase, k, n),
            device_id={"tp": to},
            device_id_type=MESH,
        ).start()

    def both(self, h, phase, k, first):
        self.push(h, phase, k, first, 0, None, 1)
        self.push(h, phase, k, first, 0, None, -1)

    def pass_on(self, h, phase, k, n):
        off = (-1, 1)[n]
        first = OFFS[k] if phase else off
        second = off if phase else 0
        self.push(h, phase, k, first, second, n, -off)

    def start(self):
        for h in (0, 1):
            self.both(h, 0, 0, 0)
        for h in (0, 1):
            self.both(h, 1, 0, 0)

    def run(self, step):
        if step == 0:
            self.start()
            return
        shards = 4 if step == 1 else 1 if step == 2 else 2
        phase = 0 if step in (2, 10) else 1
        k = step - 20 if step >= 20 else 0
        self.wait(self.buf.at[pl.ds(0, shards * self.height)], self.sem(0, phase, k, 2 if step < 10 else 0))
        for h in (0, 1):
            if step == 2:
                self.both(h, 1, 3, 2)
            elif step == 10:
                for n in (0, 1):
                    self.pass_on(h, 0, 0, n)
            elif step >= 20:
                for n in (0, 1):
                    self.pass_on(h, 1, k, n)
        if step == 10:
            for n in (0, 1):
                for h in (0, 1):
                    self.both(h, 1, n + 1, OFFS[n + 1])

    def finish(self):
        place = self.buf.at[pl.ds(0, (NTP - 1) * self.height)]
        pltpu.make_async_remote_copy(
            src_ref=place,
            dst_ref=place,
            send_sem=self.send_sem,
            recv_sem=self.sem(0, 1, 0, 2),
            device_id={"tp": self.at(0, 1)},
            device_id_type=MESH,
        ).wait_send()


class Exchange:
    def __init__(self, src, dst, send, recv, number, near):
        self.src, self.dst, self.near = src, dst, near
        self.send_sem, self.recv_sem = send.at[number], recv.at[number]
        self.me = lax.axis_index("ep")
        self.core = lax.rem(self.me, 2)
        self.rows = NEAR_SEND if near else HALF

    def block(self, ref, index):
        return ref.at[pl.ds(pl.multiple_of(index * self.rows, self.rows), self.rows)]

    def send(self, index, to, there):
        pltpu.make_async_remote_copy(
            src_ref=self.block(self.src, index),
            dst_ref=self.block(self.dst, there),
            send_sem=self.send_sem,
            recv_sem=self.recv_sem,
            device_id={"ep": to},
            device_id_type=MESH,
        ).start()

    def start(self):
        me, core = self.me, self.core
        if self.near:
            for j in (0, 1, 8, 9, 2, 3, 6, 7):
                self.send(j, lax.rem(me - core + (j - 4 + NEP), NEP), core + (8 - 2 * (j // 2)))
            self.send(5 - core, me + 1 - 2 * core, core + 4)
            own = pl.ds(pl.multiple_of((core + 4) * self.rows, self.rows), self.rows)
            self.dst[own, :] = self.src[own, :]
        else:
            for j in sorted(range(FAR), key=lambda j: abs(j // 2 - 5)):
                self.send(j, lax.rem(me - core + (j + 6), NEP), core + (20 - 2 * (j // 2)))

    def all_of(self):
        span = pl.ds(0, (NEAR - 1 if self.near else FAR) * self.rows)
        return pltpu.make_async_remote_copy(
            src_ref=self.src.at[span],
            dst_ref=self.dst.at[span],
            send_sem=self.send_sem,
            recv_sem=self.recv_sem,
            device_id={"ep": lax.rem(self.me + 1, NEP)},
            device_id_type=MESH,
        )

    def arrive(self):
        self.all_of().wait_recv()

    def finish(self):
        self.all_of().wait_send()


def iota(shape, dim):
    return lax.broadcasted_iota(jnp.int32, shape, dim)


def dot(a, b):
    return jnp.dot(a, b, preferred_element_type=F32)


def conv_span(ext, taps, cg, tp, channels, start, length):
    def group(g, carry):
        parts = []
        for u in range(2):
            rows = pl.ds(pl.multiple_of(g * 16, 16) + 8 * u, 8)
            wide = ext[rows, pl.ds(start - 128, length + 128)]
            tap = taps[rows, :]
            sums = [None] * 4
            for b in range(8):
                moved = pltpu.roll(wide, b, 1) if b else wide
                for a in range(4):
                    j = TAPS - 1 - (8 * a + b)
                    if j >= 0:
                        lane = jnp.broadcast_to(tap[:, j : j + 1], (8, 128))
                        term = jnp.concatenate([lane] * (length // 128 + 1), axis=1) * moved
                        sums[a] = term if sums[a] is None else sums[a] + term
            total = sums[0]
            for a in range(1, 4):
                total = total + pltpu.roll(sums[a], 8 * a, 1)
            parts.append(total[:, 128:])
        own = pl.ds(pl.multiple_of(tp * channels + g * 16, 16), 16)
        cg[own, :] = jnp.concatenate(parts, axis=0).astype(BF16)
        return carry

    lax.fori_loop(0, channels // 16, group, 0, unroll=UNROLL)


def kernel(
    value_hbm,
    gate_hbm,
    taps_hbm,
    gain_hbm,
    shift_hbm,
    rows_hbm,
    row_gain_hbm,
    ids_hbm,
    shares_hbm,
    ow_hbm,
    wg_hbm,
    wu_hbm,
    wd_hbm,
    mixed_ref,
    routed_ref,
    value_ref,
    gate_ref,
    taps_ref,
    gain_ref,
    shift_ref,
    rows_ref,
    row_gain_ref,
    ids_ref,
    shares_ref,
    ext,
    taps,
    tap_pad,
    tail,
    halo,
    cg_late,
    cg,
    out0,
    out1,
    outn,
    arr1,
    near,
    x0,
    x1,
    h0,
    h1,
    hn,
    y0,
    y1,
    yn,
    r0,
    r1,
    rn,
    mix,
    mixn,
    grow,
    pack_near,
    grow_near,
    ow,
    wgu,
    wd,
    load_sem,
    send,
    recv,
    zsend,
    zrecv,
    halo_sem,
):
    ep, tp = lax.axis_index("ep"), lax.axis_index("tp")
    channels, length = value_hbm.shape
    count, width = rows_hbm.shape
    cols = width // NTP

    barrier = pltpu.get_barrier_semaphore()
    y, x = tp // NX, lax.rem(tp, NX)
    for dy, dx in ((0, 1), (0, 3), (1, 0), (3, 0)):
        to = lax.rem(y + dy, NY) * NX + lax.rem(x + dx, NX)
        pl.semaphore_signal(barrier, inc=1, device_id={"tp": to}, device_id_type=MESH)

    def greet(d, carry):
        pl.semaphore_signal(
            barrier, inc=1, device_id={"ep": lax.rem(ep + d, NEP)}, device_id_type=MESH
        )
        return carry

    lax.fori_loop(1, NEP, greet, 0)

    pairs = (
        (ids_hbm, ids_ref),
        (shares_hbm, shares_ref),
        (rows_hbm, rows_ref),
        (row_gain_hbm, row_gain_ref),
        (value_hbm, value_ref),
        (gate_hbm, gate_ref),
        (taps_hbm, taps_ref),
        (gain_hbm, gain_ref),
        (shift_hbm, shift_ref),
        (ow_hbm, ow),
        (wg_hbm.at[0], wgu.at[:, pl.ds(0, cols)]),
        (wu_hbm.at[0], wgu.at[:, pl.ds(cols, cols)]),
        (wd_hbm.at[0], wd),
    )
    loads = [pltpu.make_async_copy(a, b, load_sem.at[i]) for i, (a, b) in enumerate(pairs)]
    for load in loads:
        load.start()
    for load in loads[:2]:
        load.wait()

    expert = iota((NEP, count), 0)
    chosen = jnp.zeros((NEP, count), F32)
    share = jnp.zeros((NEP, count), F32)
    for k in range(ids_ref.shape[0]):
        here = ids_ref[k : k + 1, :] == expert
        chosen = jnp.where(here, 1.0, chosen)
        share = jnp.where(here, shares_ref[k : k + 1, :], share)
    earlier = (iota((count, count), 0) < iota((count, count), 1)).astype(F32).astype(BF16)
    place = jnp.where(chosen > 0.5, dot(chosen.astype(BF16), earlier), -1.0)
    place_b = place.astype(BF16)
    for load in loads[2:4]:
        load.wait()
    total = jnp.zeros((count, cols), F32)
    for t in range(NTP):
        total = total + rows_ref[:, t * cols : (t + 1) * cols].astype(F32)
    mean = jnp.sum(total, axis=1, keepdims=True) * (1.0 / width)
    total = jnp.zeros((count, cols), F32)
    for t in range(NTP):
        off = rows_ref[:, t * cols : (t + 1) * cols].astype(F32) - mean
        total = total + off * off
    var = jnp.sum(total, axis=1, keepdims=True) * (1.0 / width)
    mine = rows_ref[:, pl.ds(pl.multiple_of(tp * cols, cols), cols)].astype(F32)
    normed = ((mine - mean) * lax.rsqrt(var + 1e-05) * row_gain_ref[pl.ds(tp, 1), :]).astype(BF16)
    base = ep - lax.rem(ep, 2)

    def owners(shape, dim, bits, first):
        owner = jnp.bitwise_and(lax.shift_right_logical(iota(shape, dim), bits) + (base + first + NEP), NEP - 1)
        return (owner == iota(shape, 1 - dim)).astype(F32).astype(BF16)

    slot_of = dot(owners((FAR_ROWS, NEP), 0, 4, 6), place_b)
    slot = jnp.bitwise_and(iota((FAR_ROWS, count), 0), HALF - 1).astype(F32)
    for c, out in enumerate((out0, out1)):
        pick = (slot_of == slot + float(HALF * c)).astype(F32).astype(BF16)
        out[...] = dot(pick, normed).astype(BF16)

    def send_near():
        shape = (NEAR * NEAR_SEND, count)
        at = dot(owners((shape[0], NEP), 0, 5, -4), place_b)
        slot = jnp.bitwise_and(iota(shape, 0), NEAR_SEND - 1).astype(F32)
        pick = (at == slot).astype(F32).astype(BF16)
        scale = lax.rsqrt(var + 1e-05)
        for t in range(0, NTP, 2):
            parts = []
            for u in (t, t + 1):
                part = (rows_ref[:, u * cols : (u + 1) * cols].astype(F32) - mean) * scale
                parts.append((part * row_gain_ref[u : u + 1, :]).astype(BF16))
            pair = dot(pick, jnp.concatenate(parts, axis=1))
            outn[:, t * cols : (t + 2) * cols] = pair.astype(BF16)
        gon.start()

    for load in loads[4:7]:
        load.wait()
    gated = (value_ref[...].astype(F32) * sigmoid(gate_ref[...].astype(F32))).astype(BF16)
    tail[...] = gated[:, length - 128 :]
    ext[:, pl.ds(128, length)] = gated.astype(F32)
    tap_pad[pl.ds(0, TAPS), pl.ds(0, channels)] = taps_ref[...]
    taps[...] = tap_pad[...].T

    pl.semaphore_wait(barrier, 4 + NEP - 1)
    halo_copy = pltpu.make_async_remote_copy(
        src_ref=tail,
        dst_ref=halo,
        send_sem=halo_sem.at[0],
        recv_sem=halo_sem.at[1],
        device_id={"ep": lax.rem(ep + 1, NEP)},
        device_id_type=MESH,
    )
    halo_copy.start()
    own = pl.ds(pl.multiple_of(tp * FAR_ROWS, 16), FAR_ROWS)
    go0 = Exchange(out0, x0.at[own], zsend, zrecv, 0, False)
    go1 = Exchange(out1, arr1, zsend, zrecv, 1, False)
    gon = Exchange(outn, near, zsend, zrecv, 2, True)
    go0.start()
    go1.start()
    half = length // 2
    conv_span(ext, taps, cg, tp, channels, 128 + half, half)
    refs = ((cg, 1), (cg_late, 1), (x0, 0), (x1, 0), (h0, 0), (h1, 0), (hn, 0))
    gathers = [TpGather(ref, send, recv, i, axis) for i, (ref, axis) in enumerate(refs)]
    back0 = Exchange(y0, r0, zsend, zrecv, 3, False)
    back1 = Exchange(y1, r1, zsend, zrecv, 4, False)
    backn = Exchange(yn, rn, zsend, zrecv, 5, True)

    def conv_late():
        halo_copy.wait_recv()
        ext[:, pl.ds(0, 128)] = jnp.where(ep > 0, halo[...].astype(F32), 0.0)
        conv_span(ext, taps, cg_late, tp, channels, 128, half)

    def halves(n):
        first = (n // 16 + 1) // 2 * 16
        return (0, first), (first, n - first)

    def wide_rows(ref, start, size):
        n = ref.shape[0] // NTP
        return jnp.concatenate([ref[t * n + start : t * n + start + size, :] for t in range(NTP)], axis=1)

    def activate(lhs):
        pre = dot(lhs, wgu[...])
        g = jnp.minimum(pre[:, :cols], 7.0)
        u = jnp.clip(pre[:, cols:], -7.0, 7.0)
        return ((u + 1.0) * g * sigmoid(1.702 * g)).astype(BF16)

    def up(xs, hs):
        n = xs.shape[0] // NTP
        for start, size in halves(n):
            own = pl.ds(pl.multiple_of(tp * n + start, 16), size)
            hs[own, :] = activate(wide_rows(xs, start, size))

    def down(hs):
        parts = [dot(wide_rows(hs, *part), wd[...]).astype(BF16) for part in halves(hs.shape[0] // NTP)]
        return jnp.concatenate(parts, axis=0)

    def moved(shape, dim, block, room):
        row = iota(shape, dim).astype(F32)
        row = row + jnp.floor((row + 0.5) * (1.0 / block)) * float(room - block)
        return (row == iota(shape, 1 - dim).astype(F32)).astype(F32).astype(BF16)

    def compact():
        go1.arrive()
        own = pl.ds(pl.multiple_of(tp * LATE_ROWS, 16), LATE_ROWS)
        x1[own, :] = dot(moved((LATE_ROWS, FAR_ROWS), 0, OTHER, HALF), arr1[...]).astype(BF16)

    def up_near():
        gon.arrive()
        room = NEAR * NEAR_SEND
        act = [activate(near[i * room // 2 : (i + 1) * room // 2, :]) for i in range(2)]
        own = pl.ds(pl.multiple_of(tp * NEAR_ROWS, 16), NEAR_ROWS)
        hn[own, :] = dot(pack_near[...], jnp.concatenate(act, axis=0)).astype(BF16)

    def return_first():
        y0[...] = down(h0)
        back0.start()

    def return_second():
        y1[...] = dot(grow[...], down(h1)).astype(BF16)
        back1.start()

    def return_near():
        yn[...] = dot(grow_near[...], down(hn)).astype(BF16)
        backn.start()

    whole = NTP * channels
    groups = whole // 128
    stride = 256

    def project_ready():
        for load in loads[7:10]:
            load.wait()
        blank = jnp.zeros((16 - groups, 128), F32)
        gains = 0.5 * jnp.concatenate([gain_ref[...], blank], axis=0).T
        shifts = 0.5 * jnp.concatenate([shift_ref[...], blank], axis=0).T
        turned = jnp.concatenate([ow[i * 128 : (i + 1) * 128, :].T for i in range(groups)], axis=1)
        return gains, shifts, turned

    def project(buf, i, first, gains, shifts, turned):
        lanes = pl.ds(i * stride, stride)
        acc = jnp.zeros((128, stride), F32)
        for t in range(groups):
            acc = acc + buf[t * 128 : (t + 1) * 128, lanes].astype(F32)
        row_mean = jnp.sum(acc, axis=0, keepdims=True) * (1.0 / whole)
        acc = jnp.zeros((128, stride), F32)
        for t in range(groups):
            off = buf[t * 128 : (t + 1) * 128, lanes].astype(F32) - row_mean
            acc = acc + off * off
        row_var = jnp.sum(acc, axis=0, keepdims=True) * (1.0 / whole)
        scale = lax.rsqrt(row_var + 1e-05)
        for t in range(groups):
            v = (buf[t * 128 : (t + 1) * 128, lanes].astype(F32) - row_mean) * scale
            v = v * gains[:, t : t + 1] + shifts[:, t : t + 1]
            buf[t * 128 : (t + 1) * 128, lanes] = (v * jnp.tanh(v) + v).astype(BF16)
        mixed = dot(turned, buf[:, lanes])
        mixed_ref[pl.ds(first + i * stride, stride), :] = mixed.T.astype(BF16)

    def turn(a):
        eye = (iota((count, count), 0) == iota((count, count), 1)).astype(F32).astype(BF16)
        return lax.dot_general(eye, a, (((1,), (1,)), ((), ())), preferred_element_type=F32).astype(BF16)

    def prepare():
        grow[...] = moved(grow.shape, 1, OTHER, HALF)
        pack_near[...] = moved(pack_near.shape, 0, SLOTS, NEAR_SEND)
        grow_near[...] = moved(grow_near.shape, 1, SLOTS, NEAR_SEND)
        share_hi = share.astype(BF16)
        share_lo = (share - share_hi.astype(F32)).astype(BF16)
        tables = [turn(a) for a in (place_b, share_hi, share_lo)]
        for columns, bits, first, out in ((FAR_ROWS, 4, 6, mix), (NEAR * NEAR_SEND, 5, -4, mixn)):
            widen = owners((NEP, columns), 1, bits, first)
            slot_at, hi_at, lo_at = [dot(a, widen) for a in tables]
            slot = jnp.bitwise_and(iota((count, columns), 1), (1 << bits) - 1).astype(F32)
            for c in range(out.shape[0] // 2):
                there = slot_at == slot + float(HALF * c)
                out[2 * c] = jnp.where(there, hi_at, 0.0).astype(BF16)
                out[2 * c + 1] = jnp.where(there, lo_at, 0.0).astype(BF16)

    def weigh(table, c, back, r):
        back.arrive()
        return dot(table[2 * c], r[...]) + dot(table[2 * c + 1], r[...])

    kept = {}

    def first_up():
        loads[10].wait()
        loads[11].wait()
        up(x0, h0)

    def first_down():
        loads[12].wait()
        return_first()

    def project_early():
        gathers[0].finish()
        kept[0] = project_ready()
        project(cg, 0, half, *kept[0])

    def project_late():
        gathers[1].finish()
        project(cg_late, 0, 0, *kept[0])

    def add(table, c, back, r):
        value = weigh(table, c, back, r)
        kept[1] = kept[1] + value if 1 in kept else value

    work = (
        conv_late,
        send_near,
        go0.arrive,
        compact,
        first_up,
        lambda: up(x1, h1),
        up_near,
        first_down,
        return_second,
        return_near,
        project_early,
        lambda: project(cg, 1, half, *kept[0]),
        project_late,
        lambda: project(cg_late, 1, 0, *kept[0]),
        prepare,
        lambda: add(mix, 0, back0, r0),
        lambda: add(mixn, 0, backn, rn),
        lambda: add(mix, 1, back1, r1),
    )
    for step in ORDER:
        if step < 900:
            gathers[step // 100].run(step % 100)
        else:
            work[step - 900]()
    routed_ref[...] = kept[1].astype(BF16)

    halo_copy.wait_send()
    for transfer in (go0, go1, gon, *gathers[2:], back0, back1, backn):
        transfer.finish()


def body(
    value_in,
    gate_in,
    conv_kernel,
    norm_gain,
    norm_shift,
    out_weight,
    expert_input,
    expert_gain,
    route_ids,
    route_weights,
    gate_weight,
    up_weight,
    down_weight,
):
    length, channels = value_in.shape
    count, width = expert_input.shape
    cols = width // NTP
    vmem = pl.BlockSpec(memory_space=pltpu.VMEM)
    hbm = pl.BlockSpec(memory_space=pltpu.HBM)
    mixed_out, routed_out = pl.pallas_call(
        kernel,
        out_shape=(
            pltpu.VMEM((length, out_weight.shape[1]), BF16),
            pltpu.VMEM((count, cols), BF16),
        ),
        in_specs=[hbm] * 13,
        out_specs=(vmem, vmem),
        scratch_shapes=[
            pltpu.VMEM((channels, length), BF16),
            pltpu.VMEM((channels, length), BF16),
            pltpu.VMEM(conv_kernel.shape, F32),
            pltpu.VMEM((NTP * channels // 128, 128), F32),
            pltpu.VMEM((NTP * channels // 128, 128), F32),
            pltpu.VMEM((count, width), BF16),
            pltpu.VMEM((NTP, cols), F32),
            pltpu.VMEM(route_ids.shape[::-1], jnp.int32),
            pltpu.VMEM(route_ids.shape[::-1], F32),
            pltpu.VMEM((channels, 128 + length), F32),
            pltpu.VMEM((128, 32), F32),
            pltpu.VMEM((32, 128), F32),
            pltpu.VMEM((channels, 128), BF16),
            pltpu.VMEM((channels, 128), BF16),
            pltpu.VMEM((NTP * channels, length // 2), BF16),
            pltpu.VMEM((NTP * channels, length // 2), BF16),
            pltpu.VMEM((FAR_ROWS, cols), BF16),
            pltpu.VMEM((FAR_ROWS, cols), BF16),
            pltpu.VMEM((NEAR * NEAR_SEND, width), BF16),
            pltpu.VMEM((FAR_ROWS, cols), BF16),
            pltpu.VMEM((NEAR * NEAR_SEND, width), BF16),
            pltpu.VMEM((NTP * FAR_ROWS, cols), BF16),
            pltpu.VMEM((NTP * LATE_ROWS, cols), BF16),
            pltpu.VMEM((NTP * FAR_ROWS, cols), BF16),
            pltpu.VMEM((NTP * LATE_ROWS, cols), BF16),
            pltpu.VMEM((NTP * NEAR_ROWS, cols), BF16),
            pltpu.VMEM((FAR_ROWS, cols), BF16),
            pltpu.VMEM((FAR_ROWS, cols), BF16),
            pltpu.VMEM((NEAR * NEAR_SEND, cols), BF16),
            pltpu.VMEM((FAR_ROWS, cols), BF16),
            pltpu.VMEM((FAR_ROWS, cols), BF16),
            pltpu.VMEM((NEAR * NEAR_SEND, cols), BF16),
            pltpu.VMEM((4, count, FAR_ROWS), BF16),
            pltpu.VMEM((2, count, NEAR * NEAR_SEND), BF16),
            pltpu.VMEM((FAR_ROWS, LATE_ROWS), BF16),
            pltpu.VMEM((NEAR_ROWS, NEAR * NEAR_SEND), BF16),
            pltpu.VMEM((NEAR * NEAR_SEND, NEAR_ROWS), BF16),
            pltpu.VMEM(out_weight.shape, BF16),
            pltpu.VMEM((width, 2 * cols), BF16),
            pltpu.VMEM((width, cols), BF16),
            pltpu.SemaphoreType.DMA((13,)),
            pltpu.SemaphoreType.DMA((7,)),
            pltpu.SemaphoreType.DMA((7 * 7,)),
            pltpu.SemaphoreType.DMA((6,)),
            pltpu.SemaphoreType.DMA((6,)),
            pltpu.SemaphoreType.DMA((2,)),
        ],
        compiler_params=pltpu.CompilerParams(
            collective_id=0, has_side_effects=True, vmem_limit_bytes=60 * 1024 * 1024
        ),
        name="whole",
    )(
        value_in.T,
        gate_in.T,
        conv_kernel,
        norm_gain.reshape(-1, 128),
        norm_shift.reshape(-1, 128),
        expert_input,
        expert_gain.reshape(NTP, cols),
        route_ids.T,
        route_weights.T,
        out_weight,
        gate_weight,
        up_weight,
        down_weight,
    )
    return (mixed_out, routed_out)


def solution(mesh):
    return jax.shard_map(
        body,
        mesh=mesh,
        in_specs=(
            P("ep", "tp"),
            P("ep", "tp"),
            P(None, "tp"),
            P(),
            P(),
            P(None, "tp"),
            P("ep", None),
            P(),
            P("ep", None),
            P("ep", None),
            P("ep", None, "tp"),
            P("ep", None, "tp"),
            P("ep", None, "tp"),
        ),
        out_specs=(P("ep", "tp"), P("ep", "tp")),
        check_vma=False,
    )
```
